32 devices in a mesh: fs: 16 (over z, y, x), tp: 2 (over core).
Axes of the slice: x: 2, y: 2, z: 4, core: 2. Of those that a mesh axis runs over, the one named last changes fastest.
Arguments:
- tokens: bfloat16 [4096, 2048], P('fs'), may hold values from -6 to 6
- mix_gain: float32 [2048], replicated, may hold values from 0.1 to 1.9
- glu_value: bfloat16 [2048, 2048], P('fs', 'tp'), may hold values from -0.125 to 0.125
- glu_gate: bfloat16 [2048, 2048], P('fs', 'tp'), may hold values from -0.125 to 0.125
- conv_taps: float32 [31, 2048], P(None, 'tp'), may hold values from -2.2 to 2.2, as said below
- chan_gain: float32 [2048], P('tp'), may hold values from 0.1 to 1.9
- mix_out: bfloat16 [2048, 2048], P('tp', 'fs'), may hold values from -0.125 to 0.125
- mlp_gain: float32 [2048], replicated, may hold values from 0.1 to 1.9
- up_weight: bfloat16 [2048, 8192], P('fs', 'tp'), may hold values from -0.125 to 0.125
- down_weight: bfloat16 [8192, 2048], P('tp', 'fs'), may hold values from -0.0625 to 0.0625
Outputs:
- result: bfloat16 [4096, 2048], P('fs')
The draws below stay inside these ranges and needn't reach their ends.
Inputs may be any that keep to these rules, and one draw needn't show every extreme that they name: `conv_taps`: independent entries scaled by fan-in; channels fall into 16 groups of different scale.
All inputs are finite; a program needn't handle non-finite values.
Results may differ from the reference program's by a relative error of at most 0.018.
Values may be sent and summed in bfloat16 or wider, within the bound.
A program may use at most 128 MiB of HBM per device.

```python
import jax
import jax.numpy as jnp
from jax import lax

D = 2048
C = 2048
FF = 8192
WIDTH = 31
LEN = 128
TOKENS = 4096
N_TP = 2


def draw_conv_taps(key, part):
    first, second = jax.random.split(key)
    raw_taps = jnp.clip(jax.random.normal(first, (WIDTH, C), jnp.float32), -4.0, 4.0)
    levels = jnp.exp(jax.random.uniform(second, (16,), jnp.float32, jnp.log(0.3), jnp.log(3.0)))
    return raw_taps * WIDTH ** (-0.5) * jnp.repeat(levels, C // 16)


def block_scale(own_key, dims, shards, smallest, largest):
    def one(position, shards_of):
        heights = jax.random.uniform(jax.random.fold_in(jax.random.fold_in(own_key, 6), position), (shards_of,), jnp.float32, smallest / len(shards), largest / len(shards))
        return jnp.repeat(jnp.exp(heights), dims[position] // shards_of).reshape((-1,) + (1,) * (len(dims) - position - 1))

    level = one(*shards[0])
    for cut in shards[1:]:
        level = level * one(*cut)
    return level


def centred(stream_key, dims, scale, limit, shards=(), held_as=jnp.bfloat16):
    values = jax.random.normal(stream_key, dims, jnp.float32) * scale
    if len(shards) > 0:
        values = block_scale(stream_key, dims, shards, -0.22, 0.18) * values
    return jnp.clip(values, min=-limit, max=limit).astype(held_as)


def setup_inputs(seed: int = 0) -> dict:
    streams_of = jax.random.split(jax.random.key(seed), 11)
    tokens = centred(streams_of[0], (TOKENS, D), 1.0, 6.0, ((0, 16),))
    mix_gain = jnp.clip(1.0 + 0.18 * jax.random.normal(streams_of[1], (D,), jnp.float32), 0.1, 1.9)
    glu_value = centred(streams_of[2], (D, C), D ** -0.5, 0.125, ((0, 16), (1, 2)))
    glu_gate = centred(streams_of[3], (D, C), D ** -0.5, 0.125, ((0, 16), (1, 2)))
    conv_taps = draw_conv_taps(jax.random.fold_in(streams_of[10], 71), 0)
    chan_gain = jnp.clip(1.0 + 0.18 * jax.random.normal(streams_of[5], (C,), jnp.float32), 0.1, 1.9)
    mix_out = centred(streams_of[6], (C, D), C ** -0.5, 0.125, ((0, 2), (1, 16)))
    mlp_gain = jnp.clip(1.0 + 0.18 * jax.random.normal(streams_of[7], (D,), jnp.float32), 0.1, 1.9)
    up_weight = centred(streams_of[8], (D, FF), D ** -0.5, 0.125, ((0, 16), (1, 2)))
    down_weight = centred(streams_of[9], (FF, D), FF ** -0.5, 0.0625, ((0, 2), (1, 16)))
    return {"tokens": tokens, "mix_gain": mix_gain, "glu_value": glu_value, "glu_gate": glu_gate, "conv_taps": conv_taps, "chan_gain": chan_gain, "mix_out": mix_out, "mlp_gain": mlp_gain, "up_weight": up_weight, "down_weight": down_weight}


norm_floor = 0.05

def rms_scale(stream, gain):
    return stream * lax.rsqrt(lax.optimization_barrier(jnp.mean(stream * stream, axis=-1, keepdims=True)) + norm_floor) * gain

def bf16_round(value):
    return lax.optimization_barrier(value.astype(jnp.bfloat16)).astype(jnp.float32)

def depthwise(glu, conv_taps):
    seqs = glu.shape[0] // LEN
    blocks = glu.reshape(seqs, LEN, glu.shape[1]).astype(jnp.float32)
    reach = conv_taps.shape[0] // 2
    padded = jnp.pad(blocks, ((0, 0), (reach, reach), (0, 0)))
    total = jnp.zeros_like(blocks)
    for offset in range(conv_taps.shape[0]):
        total = total + padded[:, offset:offset + LEN] * conv_taps[offset]
    return total.reshape(glu.shape)

def shard_sum(left, right):
    block = left.shape[1] // N_TP
    total = jnp.zeros((left.shape[0], right.shape[1]), jnp.float32)
    for shard in range(N_TP):
        partial_term = jnp.dot(left[:, shard * block:(shard + 1) * block], right[shard * block:(shard + 1) * block], preferred_element_type=jnp.float32)
        total = total + bf16_round(partial_term)
    return total.astype(jnp.bfloat16)

def reference(tokens, mix_gain, glu_value, glu_gate, conv_taps, chan_gain, mix_out, mlp_gain, up_weight, down_weight):
    stream = tokens.astype(jnp.float32)
    normed = rms_scale(stream, mix_gain).astype(jnp.bfloat16)
    values = jnp.dot(normed, glu_value, preferred_element_type=jnp.float32)
    gating = jnp.dot(normed, glu_gate, preferred_element_type=jnp.float32)
    glu = (values * jax.nn.sigmoid(gating)).astype(jnp.bfloat16)
    convolved = depthwise(glu, conv_taps)
    centre = lax.optimization_barrier(jnp.mean(convolved, axis=-1, keepdims=True))
    spread = lax.optimization_barrier(jnp.mean(convolved * convolved, axis=-1, keepdims=True)) - centre * centre
    hidden = jax.nn.silu((convolved - centre) * lax.rsqrt(spread + norm_floor) * chan_gain).astype(jnp.bfloat16)
    mixed = shard_sum(hidden, mix_out)
    resid = stream + mixed.astype(jnp.float32)
    normed_mlp = rms_scale(resid, mlp_gain).astype(jnp.bfloat16)
    active = jnp.square(jax.nn.relu(jnp.dot(normed_mlp, up_weight, preferred_element_type=jnp.float32))).astype(jnp.bfloat16)
    feed = shard_sum(active, down_weight)
    return (resid + feed.astype(jnp.float32)).astype(jnp.bfloat16)
```

```python
import functools

import jax
import jax.numpy as jnp
from jax import lax
from jax.experimental import pallas as pl
from jax.experimental.pallas import tpu as pltpu
from jax.sharding import PartitionSpec as P

C = 2048
LEN = 128


norm_floor = 0.05


def rms_scale(stream, gain):
    return stream * lax.rsqrt(jnp.mean(stream * stream, axis=-1, keepdims=True) + norm_floor) * gain


def bf16_round(value):
    return lax.optimization_barrier(value.astype(jnp.bfloat16)).astype(jnp.float32)


def depthwise(glu, conv_taps):
    seqs = glu.shape[0] // LEN
    blocks = glu.reshape(seqs, LEN, glu.shape[1]).astype(jnp.float32)
    reach = conv_taps.shape[0] // 2
    padded = jnp.pad(blocks, ((0, 0), (reach, reach), (0, 0)))
    total = jnp.zeros_like(blocks)
    for offset in range(conv_taps.shape[0]):
        total = total + padded[:, offset : offset + LEN] * conv_taps[offset]
    return total.reshape(glu.shape)


def swap_then_gather(weight, inner, outer, split, join):
    own = lax.all_to_all(
        weight, "fs", split_axis=split, concat_axis=join, axis_index_groups=inner, tiled=True
    )
    return lax.all_gather(own, "fs", axis=join, axis_index_groups=outer, tiled=True)


def shared_sum(partial, inner, tp):
    part = lax.all_to_all(
        partial, "fs", split_axis=0, concat_axis=0, axis_index_groups=inner, tiled=True
    )
    group = len(inner[0])
    rows = partial.shape[0] // group
    part = part.reshape(group, tp, rows // tp, -1).transpose(1, 0, 2, 3)
    part = lax.all_to_all(part, "tp", split_axis=0, concat_axis=0, tiled=True)
    return bf16_round(jnp.sum(part.astype(jnp.float32), axis=(0, 1)))


def plain_device(
    tokens,
    mix_gain,
    glu_value,
    glu_gate,
    conv_taps,
    chan_gain,
    mix_out,
    mlp_gain,
    up_weight,
    down_weight,
):
    fs, tp = lax.axis_size("fs"), lax.axis_size("tp")
    group = 4 if fs % 4 == 0 else 1
    inner = [[o * group + i for i in range(group)] for o in range(fs // group)]
    outer = [[o * group + i for o in range(fs // group)] for i in range(group)]
    place = lax.rem(lax.axis_index("fs"), group)

    value_w = swap_then_gather(glu_value, inner, outer, 1, 0)
    gate_w = swap_then_gather(glu_gate, inner, outer, 1, 0)
    mix_w = swap_then_gather(mix_out, inner, outer, 0, 1)
    up_w = swap_then_gather(up_weight, inner, outer, 1, 0)
    down_w = swap_then_gather(down_weight, inner, outer, 0, 1)

    stream = tokens.astype(jnp.float32)
    normed = rms_scale(stream, mix_gain).astype(jnp.bfloat16)
    normed = lax.all_gather(normed, "fs", axis=0, axis_index_groups=inner, tiled=True)
    values = jnp.dot(normed, value_w, preferred_element_type=jnp.float32)
    gating = jnp.dot(normed, gate_w, preferred_element_type=jnp.float32)
    glu = (values * jax.nn.sigmoid(gating)).astype(jnp.bfloat16)
    channels = value_w.shape[1]
    taps = lax.dynamic_slice_in_dim(conv_taps, place * channels, channels, 1)
    gain = lax.dynamic_slice_in_dim(chan_gain, place * channels, channels, 0)
    convolved = depthwise(glu, taps)
    both = jnp.stack(
        (jnp.sum(convolved, axis=-1), jnp.sum(convolved * convolved, axis=-1))
    )
    both = jnp.sum(lax.all_gather(both, "fs", axis=0, axis_index_groups=inner), axis=0)
    both = lax.psum(both, "tp")
    centre = (both[0] / C)[:, None]
    spread = (both[1] / C)[:, None] - centre * centre
    hidden = jax.nn.silu((convolved - centre) * lax.rsqrt(spread + norm_floor) * gain).astype(
        jnp.bfloat16
    )
    mixed = shared_sum(
        jnp.dot(hidden, mix_w, preferred_element_type=jnp.float32).astype(jnp.bfloat16), inner, tp
    )
    own_rows = stream.shape[0] // tp
    own_stream = lax.dynamic_slice_in_dim(stream, lax.axis_index("tp") * own_rows, own_rows, 0)
    resid = own_stream + mixed
    normed_mlp = rms_scale(resid, mlp_gain).astype(jnp.bfloat16)
    normed_mlp = lax.all_gather(normed_mlp, "fs", axis=0, axis_index_groups=inner)
    normed_mlp = lax.all_gather(normed_mlp, "tp", axis=1).reshape(-1, normed.shape[1])
    active = jnp.square(
        jax.nn.relu(jnp.dot(normed_mlp, up_w, preferred_element_type=jnp.float32))
    ).astype(jnp.bfloat16)
    feed = shared_sum(
        jnp.dot(active, down_w, preferred_element_type=jnp.float32).astype(jnp.bfloat16), inner, tp
    )
    finished = (resid + feed).astype(jnp.bfloat16)
    return lax.all_gather(finished, "tp", axis=0, tiled=True)

MESH = pl.DeviceIdType.MESH
F32, BF16 = jnp.float32, jnp.bfloat16


def rows_at(start, size):
    return pl.ds(pl.multiple_of(start, 128), size)


def layer_kernel(
    ng,
    tok, mixg, gv, gg, taps, chg, mo, mlpg, up, dn,
    out,
    fgv, fgg, fmo, fup, fdn,
    nrm, pad, cv, hid, st, st_all,
    acc, resid, nm_all, act, fin,
    sbo1, sbi1, rdo1, rdi1, sbo2, sbi2, rdo2, rdi2,
    ws, wr, lsem, tsem, nsem, ssem, rsem, fsem,
):
    f, t = lax.axis_index("fs"), lax.axis_index("tp")
    x, y = lax.rem(f, 2), lax.rem(lax.div(f, 2), 2)
    zp, zh = lax.rem(lax.div(f, 4), 2), lax.div(f, 8)
    mid = lax.rem(zp + zh, 2)
    sib = 1 - t
    L = tok.shape[0] // 2
    half = ng * L
    width = tok.shape[1]
    chans = fgv.shape[1]
    hidden = fup.shape[1]
    depth = gv.shape[0]
    sends, sent = [], set()

    def flip(coord, bit):
        return 1 - coord if bit else coord

    def chip(dq):
        return flip(mid, dq // 2) * 2 + flip(x, dq % 2)

    def fs_of(dq, do):
        return flip(zh, do // 2) * 8 + flip(zp, (dq // 2 + do // 2) % 2) * 4 + flip(y, do % 2) * 2 + flip(x, dq % 2)

    def seat(dq):
        return flip(y, dq // 2) * 2 + flip(x, dq % 2)

    def seat_fs(dq, do=0):
        return zh * 8 + zp * 4 + flip(y, dq // 2) * 2 + flip(x, dq % 2)

    p, s = chip(0), seat(0)
    near, mate = fs_of(2, 0), fs_of(0, 2)
    z = zh * 2 + zp
    z_near = zh * 2 + 1 - zp
    z_mate, z_far = (1 - zh) * 2 + zh, (1 - zh) * 2 + 1 - zh
    outer, inner = mid == 0, mid == 1

    def remote(src, dst, s_sem, r_sem, device):
        return pltpu.make_async_remote_copy(
            src_ref=src, dst_ref=dst, send_sem=s_sem, recv_sem=r_sem,
            device_id=device, device_id_type=MESH,
        )

    def act_if(when, act):
        if when is None:
            act()
        else:
            pl.when(when)(act)

    def start(src, dst, s_sem, r_sem, device, when=None):
        copy = remote(src, dst, s_sem, r_sem, device)
        act_if(when, copy.start)
        return copy

    def push(src, dst, s_sem, r_sem, device, when=None):
        sends.append((start(src, dst, s_sem, r_sem, device, when), when))

    def once(key, copy):
        if key not in sent:
            sent.add(key)
            sends.append((copy, None))

    def arrived(dst, s_sem, r_sem):
        remote(dst, dst, s_sem, r_sem, (f, sib)).wait_recv()

    barrier = pltpu.get_barrier_semaphore()
    peers = [(seat_fs(dq), u) for dq in range(1, ng) for u in (t, sib)]
    peers += [(f, sib), (near, t), (fs_of(3, 0), t), (mate, t)]
    for peer in peers:
        pl.semaphore_signal(barrier, inc=1, device_id=peer, device_id_type=MESH)
    pl.semaphore_wait(barrier, len(peers))

    weights = (
        (lambda q: gv.at[:, rows_at(q * chans, chans)], lambda g: fgv.at[rows_at(g * depth, depth), :]),
        (lambda q: gg.at[:, rows_at(q * chans, chans)], lambda g: fgg.at[rows_at(g * depth, depth), :]),
        (lambda q: mo.at[rows_at(q * chans, chans), :], lambda g: fmo.at[:, rows_at(g * depth, depth)]),
        (lambda q: up.at[:, rows_at(q * hidden, hidden)], lambda g: fup.at[rows_at(g * depth, depth), :]),
        (lambda q: dn.at[rows_at(q * hidden, hidden), :], lambda g: fdn.at[:, rows_at(g * depth, depth)]),
    )

    def spread_in_plane(a, which=(1, 2, 3), when=None):
        src, dst = weights[a]
        part, place = (seat, seat_fs) if a < 3 else (chip, fs_of)
        for dq in which:
            copy = start(src(part(dq)), dst(f), ws.at[a, dq], wr.at[a, dq], (place(dq, 0), t), when)
            once((a, 0, dq), copy)

    def send(a, do, which=(0, 1, 2, 3), when=None):
        src, dst = weights[a]
        for dq in which:
            piece = dst(fs_of(dq, 0))
            copy = start(
                src(p) if dq == 0 else piece, piece,
                ws.at[a, do * ng + dq], wr.at[a, do * ng + dq], (fs_of(0, do), t), when,
            )
            once((a, do, dq), copy)

    def got(a, dq, when=None):
        piece = weights[a][1]((seat_fs if a < 3 else fs_of)(dq, 0))
        come = remote(piece, piece, ws.at[a, 0], wr.at[a, dq], (f, sib))
        act_if(when, come.wait_recv)

    def got_and_send(a, which, when=None, zh_when=None):
        for dq in which:
            got(a, dq, when)
            send(a, 1, (dq,), when)
            if zh_when is not None:
                send(a, 2, (dq,), zh_when)

    def relay(a, which=(0, 1, 2, 3), when=None):
        dst = weights[a][1]
        for dq in which:
            piece = dst(fs_of(dq, 2))
            come = remote(piece, piece, ws.at[a, 0], wr.at[a, 2 * ng + dq], (f, sib))
            copy = remote(piece, piece, ws.at[a, 3 * ng + dq], wr.at[a, 3 * ng + dq], (fs_of(0, 1), t))

            def pass_on():
                come.wait_recv()
                copy.start()

            act_if(when, pass_on)
            once((a, 3, dq), copy)

    def whole(a):
        dst = weights[a][1]
        for do in (1, 3):
            for dq in range(ng):
                arrived(dst(fs_of(dq, do)), ws.at[a, 0], wr.at[a, do * ng + dq])
        local(a).wait()

    def local(a):
        src, dst = weights[a]
        return pltpu.make_async_copy(src(s if a < 3 else p), dst(f), lsem.at[a])

    planes = (
        lambda g: fgv.at[rows_at(g * ng * depth, ng * depth), :],
        lambda g: fgg.at[rows_at(g * ng * depth, ng * depth), :],
        lambda g: fmo.at[:, rows_at(g * ng * depth, ng * depth)],
    )

    def line(a, g, s_at, r_at, to, when=None):
        block = planes[a](g)
        push(block, block, ws.at[a, s_at], wr.at[a, r_at], (to, t), when)

    def line_got(a, g, r_at, when):
        come = remote(planes[a](g), planes[a](g), ws.at[a, 0], wr.at[a, r_at], (f, sib))
        act_if(when, come.wait_recv)

    def line_own(a, when=None):
        line(a, z, 4, 4, near, when)
        if when is not outer:
            line(a, z, 7, 5, mate, inner)

    def line_near(a):
        line_got(a, z_near, 4, inner)
        line(a, z_near, 8, 6, mate, inner)

    def line_mate(a):
        line_got(a, z_mate, 5, inner)
        line(a, z_mate, 5, 5, near, inner)

    def line_far(a):
        line_got(a, z_far, 6, inner)
        line(a, z_far, 6, 6, near, inner)

    def line_whole(a):
        for g, r_at in ((z_near, 4), (z_mate, 5), (z_far, 6)):
            line_got(a, g, r_at, outer)

    first = (nrm, tsem, seat, seat_fs)
    second = (nm_all, nsem, chip, fs_of)

    def gather_start(buf, sem, part, place):
        own = buf.at[rows_at(t * half + part(0) * L, L)]
        for dq in (2, 1):
            push(own, own, sem.at[0, dq], sem.at[1, dq], (place(dq, 0), t))
        push(own, own, sem.at[2, 0], sem.at[3, 0], (f, sib))

    def gather_relay(rows, *which):
        buf, sem, part, place = rows
        for dq in which:
            block = buf.at[rows_at(t * half + part(dq) * L, L)]
            arrived(block, sem.at[0, 0], sem.at[1, dq])
            if dq == 2:
                push(block, block, sem.at[0, 3], sem.at[1, 3], (place(1, 0), t))
            push(block, block, sem.at[2, dq], sem.at[3, dq], (f, sib))

    def gather_finish(rows, *which):
        buf, sem, part, place = rows
        for dq in which:
            arrived(buf.at[rows_at(sib * half + part(dq) * L, L)], sem.at[0, 0], sem.at[3, dq])

    step = 16

    def norm_rows(load, gain, dst, start):
        def body(i, _):
            value = load(i * step).astype(F32)
            scale = lax.rsqrt(jnp.mean(value * value, axis=-1, keepdims=True) + norm_floor)
            dst[pl.ds(pl.multiple_of(start + i * step, step), step), :] = (
                value * scale * gain[...]
            ).astype(BF16)
            return 0

        lax.fori_loop(0, L // step, body, 0)

    def from_ref(ref, base):
        return lambda i: ref[pl.ds(pl.multiple_of(base + i, step), step), :]

    for a in (0, 1):
        spread_in_plane(a)
    for a in range(5):
        local(a).start()
    norm_rows(from_ref(tok, t * L), mixg, nrm, t * half + s * L)
    gather_start(*first)
    spread_in_plane(2)

    def plane_ready(a):
        for dq in (1, 2, 3):
            got(a, dq)
        local(a).wait()

    for a in (0, 1):
        plane_ready(a)
        line_own(a)
    gather_relay(first, 2, 1)
    for a in (3, 4):
        spread_in_plane(a, (1,))
        send(a, 1, (0,))
    for step_of in (line_near, line_mate):
        for a in (0, 1):
            step_of(a)
    plane_ready(2)
    line_own(2, outer)
    for a in (0, 1):
        line_far(a)
    line_own(2, inner)
    line_near(2)
    send(3, 2, (0,), inner)
    spread_in_plane(3, (3, 2), outer)
    gather_finish(first, 0, 1)
    for a in (0, 1):
        line_whole(a)
    pad[...] = jnp.zeros_like(pad)
    st[...] = jnp.zeros_like(st)
    taps_n = taps.shape[0]
    reach = taps_n // 2
    lead = (reach + 7) // 8 * 8
    own_cols = s * chans
    eye = lax.broadcasted_iota(jnp.int32, (L, L), 0) == lax.broadcasted_iota(jnp.int32, (L, L), 1)

    def conv_block(i, _):
        b = lax.rem(i, 2) * ng + lax.rem(y + lax.div(i, 4), 2) * 2 + lax.rem(x + lax.div(i, 2), 2)
        rows = rows_at(b * L, L)
        left = nrm[rows, :]
        values = jnp.dot(left, fgv[...], preferred_element_type=F32)
        gating = jnp.dot(left, fgg[...], preferred_element_type=F32)
        glu = (values * jax.nn.sigmoid(gating)).astype(BF16).astype(F32)
        pad[pl.ds(lead, L), :] = glu
        sums = jnp.zeros((L, 1), F32)
        squares = jnp.zeros((L, 1), F32)
        for c in range(chans // 128):
            total = jnp.zeros((L, 128), F32)
            for j in range(taps_n):
                tap = taps[pl.ds(j, 1), rows_at(own_cols + c * 128, 128)]
                total = total + pad[pl.ds(lead - reach + j, L), pl.ds(c * 128, 128)] * tap
            cv[rows, pl.ds(c * 128, 128)] = total
            sums = sums + jnp.sum(total, axis=1, keepdims=True)
            squares = squares + jnp.sum(total * total, axis=1, keepdims=True)
        st[b, pl.ds(0, 1), :] = jnp.sum(jnp.where(eye, sums, 0.0), axis=0, keepdims=True)
        st[b, pl.ds(1, 1), :] = jnp.sum(jnp.where(eye, squares, 0.0), axis=0, keepdims=True)
        return 0

    lax.fori_loop(0, ng, conv_block, 0)
    gather_relay(first, 3)
    line_mate(2)
    got_and_send(3, (1,), None, inner)
    spread_in_plane(4, (3, 2), outer)
    gather_finish(first, 2, 3)
    lax.fori_loop(ng, 2 * ng, conv_block, 0)

    slots = [(dq, du) for dq in range(ng) for du in range(2) if (dq, du) != (0, 0)]
    for dq, du in slots:
        push(
            st, st_all.at[dq * 2 + du],
            ssem.at[0, dq * 2 + du], ssem.at[1, dq * 2 + du],
            (seat_fs(dq), t if du == 0 else sib),
        )
    line_far(2)
    spread_in_plane(3, (3, 2), inner)
    spread_in_plane(4, (3, 2), inner)
    send(4, 2, (0,), inner)
    got_and_send(4, (1,), None, inner)
    for dq, du in slots:
        arrived(st_all.at[dq * 2 + du], ssem.at[0, 0], ssem.at[1, dq * 2 + du])

    def hidden_block(b, _):
        rows = rows_at(b * L, L)
        total = st[b]
        for dq, du in slots:
            total = total + st_all[dq * 2 + du, b]
        count = chans * ng * 2
        sums = jnp.sum(jnp.where(eye, total[0:1, :], 0.0), axis=1, keepdims=True)
        squares = jnp.sum(jnp.where(eye, total[1:2, :], 0.0), axis=1, keepdims=True)
        centre = sums / count
        spread = squares / count - centre * centre
        value = (cv[rows, :] - centre) * lax.rsqrt(spread + norm_floor)
        value = value * chg[:, rows_at(own_cols, chans)]
        hid[rows, :] = (value * jax.nn.sigmoid(value)).astype(BF16)
        return 0

    lax.fori_loop(0, 2 * ng, hidden_block, 0)

    cols = 512

    def reduce_rows(left, right, sbo, sbi, rdo, rdi, k, part, place, between=lambda: None):
        def theirs(n, _):
            at = rows_at(n * cols, cols)
            sbo[:, at] = jnp.dot(
                left[rows_at(sib * half, half), :], right[:, at], preferred_element_type=F32
            ).astype(BF16)
            return 0

        lax.fori_loop(0, width // cols, theirs, 0)
        push(sbo, sbi, rsem.at[k, 0], rsem.at[k, 1], (f, sib))

        def mine(n, _):
            at = rows_at(n * cols, cols)
            acc[:, at] = jnp.dot(
                left[rows_at(t * half, half), :], right[:, at], preferred_element_type=F32
            )
            return 0

        lax.fori_loop(0, width // cols, mine, 0)
        arrived(sbi, rsem.at[k, 0], rsem.at[k, 1])
        for dq in (3, 1, 2):
            base = part(dq) * L
            if dq == 2:
                between()
                arrived(rdi.at[2], rsem.at[k, 0], rsem.at[k, 7])

            def add(i, _):
                at = pl.ds(pl.multiple_of(base + i * step, step), step)
                total = acc[at, :] + sbi[at, :].astype(F32)
                if dq == 2:
                    total = total + rdi[2, pl.ds(pl.multiple_of(i * step, step), step), :].astype(F32)
                rdo[at, :] = total.astype(BF16)
                return 0

            lax.fori_loop(0, L // step, add, 0)
            push(
                rdo.at[rows_at(base, L)], rdi.at[dq - 1],
                rsem.at[k, 2 * dq], rsem.at[k, 2 * dq + 1], (place(2 if dq == 2 else 1, 0), t),
            )

    def reduced(sbi, rdi, own, i):
        at = pl.ds(pl.multiple_of(own * L + i * step, step), step)
        total = acc[at, :] + sbi[at, :].astype(F32)
        for dq in (1, 2):
            total = total + rdi[dq - 1, pl.ds(pl.multiple_of(i * step, step), step), :].astype(F32)
        return total.astype(BF16).astype(F32)

    def wait_reduced(rdi, k):
        for dq in (1, 2):
            arrived(rdi.at[dq - 1], rsem.at[k, 0], rsem.at[k, 2 * dq + 1])

    line_whole(2)

    def before_partial():
        send(3, 2, (0,), outer)
        got_and_send(3, (2, 3), None, inner)

    reduce_rows(hid, fmo, sbo1, sbi1, rdo1, rdi1, 0, seat, seat_fs, before_partial)
    send(3, 2, (1, 2, 3), outer)
    relay(3, when=inner)
    got_and_send(4, (2, 3), inner, inner)
    wait_reduced(rdi1, 0)

    def resid_rows(i, _):
        at = pl.ds(pl.multiple_of(i * step, step), step)
        own = tok[pl.ds(pl.multiple_of(t * L + i * step, step), step), :].astype(F32)
        value = own + reduced(sbi1, rdi1, s, i)
        resid[at, :] = value
        scale = lax.rsqrt(jnp.mean(value * value, axis=-1, keepdims=True) + norm_floor)
        nm_all[pl.ds(pl.multiple_of(t * half + p * L + i * step, step), step), :] = (
            value * scale * mlpg[...]
        ).astype(BF16)
        return 0

    lax.fori_loop(0, L // step, resid_rows, 0)
    gather_start(*second)
    relay(3, when=outer)
    gather_relay(second, 2)
    got_and_send(4, (2, 3), outer)
    send(4, 2, when=outer)
    relay(4, (0, 1), inner)
    gather_relay(second, 1, 3)
    relay(4, (2, 3), inner)

    whole(3)

    def up_half(u):
        def body(n, _):
            at = rows_at(n * 256, 256)
            value = jnp.dot(
                nm_all[rows_at(u * half, half), :], fup[:, at], preferred_element_type=F32
            )
            value = jnp.maximum(value, 0.0)
            act[rows_at(u * half, half), at] = (value * value).astype(BF16)
            return 0

        lax.fori_loop(0, hidden // 256, body, 0)

    up_half(t)
    gather_finish(second, 0, 1, 2, 3)
    up_half(sib)
    relay(4, when=outer)
    whole(4)
    reduce_rows(act, fdn, sbo2, sbi2, rdo2, rdi2, 1, chip, fs_of)
    wait_reduced(rdi2, 1)

    def finish_rows(i, _):
        at = pl.ds(pl.multiple_of(i * step, step), step)
        value = (resid[at, :] + reduced(sbi2, rdi2, p, i)).astype(BF16)
        fin[0, at, :] = value
        out[pl.ds(pl.multiple_of(t * L + i * step, step), step), :] = value
        return 0

    lax.fori_loop(0, L // step, finish_rows, 0)
    push(fin.at[0], fin.at[1], fsem.at[0], fsem.at[1], (f, sib))
    arrived(fin.at[1], fsem.at[0], fsem.at[1])

    def copy_rows(i, _):
        at = pl.ds(pl.multiple_of(i * step, step), step)
        out[pl.ds(pl.multiple_of(sib * L + i * step, step), step), :] = fin[1, at, :]
        return 0

    lax.fori_loop(0, L // step, copy_rows, 0)
    for copy, when in sends:
        act_if(when, copy.wait_send)


def fused_device(ng, nz, tokens, mix_gain, glu_value, glu_gate, conv_taps, chan_gain, mix_out, mlp_gain, up_weight, down_weight):
    rows, width = tokens.shape
    fs = ng * nz
    L = rows // 2
    half = ng * L
    chans = glu_value.shape[1] // ng
    hidden = up_weight.shape[1] // ng
    depth = glu_value.shape[0]
    blocks = 2 * ng
    vm = pltpu.VMEM
    dma = pltpu.SemaphoreType.DMA
    reduce_bufs = [
        vm((half, width), BF16), vm((half, width), BF16), vm((half, width), BF16),
        vm((ng - 1, L, width), BF16),
    ]
    scratch = [
        vm((fs * depth, chans), BF16), vm((fs * depth, chans), BF16), vm((chans, width), BF16),
        vm((fs * depth, hidden), BF16), vm((hidden, width), BF16),
        vm((2 * half, width), BF16),
        vm((L + 32, chans), F32), vm((2 * half, chans), F32), vm((2 * half, chans), BF16),
        vm((blocks, 8, L), F32), vm((blocks, blocks, 8, L), F32),
        vm((half, width), F32), vm((L, width), F32), vm((2 * half, width), BF16),
        vm((2 * half, hidden), BF16), vm((2, L, width), BF16),
        *reduce_bufs, *reduce_bufs,
        dma((5, fs)), dma((5, fs)), dma((5,)), dma((4, ng)), dma((4, ng)),
        dma((2, blocks)), dma((2, 2 * ng)), dma((2,)),
    ]
    return pl.pallas_call(
        functools.partial(layer_kernel, ng),
        out_shape=jax.ShapeDtypeStruct((rows, width), BF16),
        in_specs=[pl.BlockSpec(memory_space=vm)] * 10,
        out_specs=pl.BlockSpec(memory_space=vm),
        scratch_shapes=scratch,
        compiler_params=pltpu.CompilerParams(
            collective_id=0, has_side_effects=True, vmem_limit_bytes=60 * 1024 * 1024
        ),
    )(
        tokens, mix_gain[None], glu_value, glu_gate, conv_taps, chan_gain[None], mix_out,
        mlp_gain[None], up_weight, down_weight,
    )


def per_device(*args):
    tokens, glu_value, conv_taps = args[0], args[2], args[4]
    fs, tp = lax.axis_size("fs"), lax.axis_size("tp")
    group = 4
    fits = (
        tp == 2
        and fs == group * 4
        and tokens.shape[0] == 2 * LEN
        and glu_value.shape[0] % 128 == 0
        and conv_taps.shape[1] % (group * 128) == 0
        and conv_taps.shape[0] <= 31
    )
    if fits:
        return fused_device(group, fs // group, *args)
    return plain_device(*args)


def solution(mesh):
    in_specs = (
        P("fs", None),
        P(),
        P("fs", "tp"),
        P("fs", "tp"),
        P(None, "tp"),
        P("tp"),
        P("tp", "fs"),
        P(),
        P("fs", "tp"),
        P("tp", "fs"),
    )
    out_specs = P("fs", None)
    return jax.shard_map(
        per_device, mesh=mesh, in_specs=in_specs, out_specs=out_specs, check_vma=False
    )
```

```python
import functools

import jax
import jax.numpy as jnp
from jax import lax
from jax.experimental import pallas as pl
from jax.experimental.pallas import tpu as pltpu
from jax.sharding import PartitionSpec as P

C = 2048
LEN = 128


norm_floor = 0.05


def rms_scale(stream, gain):
    return stream * lax.rsqrt(jnp.mean(stream * stream, axis=-1, keepdims=True) + norm_floor) * gain


def bf16_round(value):
    return lax.optimization_barrier(value.astype(jnp.bfloat16)).astype(jnp.float32)


def depthwise(glu, conv_taps):
    seqs = glu.shape[0] // LEN
    blocks = glu.reshape(seqs, LEN, glu.shape[1]).astype(jnp.float32)
    reach = conv_taps.shape[0] // 2
    padded = jnp.pad(blocks, ((0, 0), (reach, reach), (0, 0)))
    total = jnp.zeros_like(blocks)
    for offset in range(conv_taps.shape[0]):
        total = total + padded[:, offset : offset + LEN] * conv_taps[offset]
    return total.reshape(glu.shape)


def swap_then_gather(weight, inner, outer, split, join):
    own = lax.all_to_all(
        weight, "fs", split_axis=split, concat_axis=join, axis_index_groups=inner, tiled=True
    )
    return lax.all_gather(own, "fs", axis=join, axis_index_groups=outer, tiled=True)


def shared_sum(partial, inner, tp):
    part = lax.all_to_all(
        partial, "fs", split_axis=0, concat_axis=0, axis_index_groups=inner, tiled=True
    )
    group = len(inner[0])
    rows = partial.shape[0] // group
    part = part.reshape(group, tp, rows // tp, -1).transpose(1, 0, 2, 3)
    part = lax.all_to_all(part, "tp", split_axis=0, concat_axis=0, tiled=True)
    return bf16_round(jnp.sum(part.astype(jnp.float32), axis=(0, 1)))


def plain_device(
    tokens,
    mix_gain,
    glu_value,
    glu_gate,
    conv_taps,
    chan_gain,
    mix_out,
    mlp_gain,
    up_weight,
    down_weight,
):
    fs, tp = lax.axis_size("fs"), lax.axis_size("tp")
    group = 4 if fs % 4 == 0 else 1
    inner = [[o * group + i for i in range(group)] for o in range(fs // group)]
    outer = [[o * group + i for o in range(fs // group)] for i in range(group)]
    place = lax.rem(lax.axis_index("fs"), group)

    value_w = swap_then_gather(glu_value, inner, outer, 1, 0)
    gate_w = swap_then_gather(glu_gate, inner, outer, 1, 0)
    mix_w = swap_then_gather(mix_out, inner, outer, 0, 1)
    up_w = swap_then_gather(up_weight, inner, outer, 1, 0)
    down_w = swap_then_gather(down_weight, inner, outer, 0, 1)

    stream = tokens.astype(jnp.float32)
    normed = rms_scale(stream, mix_gain).astype(jnp.bfloat16)
    normed = lax.all_gather(normed, "fs", axis=0, axis_index_groups=inner, tiled=True)
    values = jnp.dot(normed, value_w, preferred_element_type=jnp.float32)
    gating = jnp.dot(normed, gate_w, preferred_element_type=jnp.float32)
    glu = (values * jax.nn.sigmoid(gating)).astype(jnp.bfloat16)
    channels = value_w.shape[1]
    taps = lax.dynamic_slice_in_dim(conv_taps, place * channels, channels, 1)
    gain = lax.dynamic_slice_in_dim(chan_gain, place * channels, channels, 0)
    convolved = depthwise(glu, taps)
    both = jnp.stack(
        (jnp.sum(convolved, axis=-1), jnp.sum(convolved * convolved, axis=-1))
    )
    both = jnp.sum(lax.all_gather(both, "fs", axis=0, axis_index_groups=inner), axis=0)
    both = lax.psum(both, "tp")
    centre = (both[0] / C)[:, None]
    spread = (both[1] / C)[:, None] - centre * centre
    hidden = jax.nn.silu((convolved - centre) * lax.rsqrt(spread + norm_floor) * gain).astype(
        jnp.bfloat16
    )
    mixed = shared_sum(
        jnp.dot(hidden, mix_w, preferred_element_type=jnp.float32).astype(jnp.bfloat16), inner, tp
    )
    own_rows = stream.shape[0] // tp
    own_stream = lax.dynamic_slice_in_dim(stream, lax.axis_index("tp") * own_rows, own_rows, 0)
    resid = own_stream + mixed
    normed_mlp = rms_scale(resid, mlp_gain).astype(jnp.bfloat16)
    normed_mlp = lax.all_gather(normed_mlp, "fs", axis=0, axis_index_groups=inner)
    normed_mlp = lax.all_gather(normed_mlp, "tp", axis=1).reshape(-1, normed.shape[1])
    active = jnp.square(
        jax.nn.relu(jnp.dot(normed_mlp, up_w, preferred_element_type=jnp.float32))
    ).astype(jnp.bfloat16)
    feed = shared_sum(
        jnp.dot(active, down_w, preferred_element_type=jnp.float32).astype(jnp.bfloat16), inner, tp
    )
    finished = (resid + feed).astype(jnp.bfloat16)
    return lax.all_gather(finished, "tp", axis=0, tiled=True)

MESH = pl.DeviceIdType.MESH
F32, BF16 = jnp.float32, jnp.bfloat16


OUTER = (
    ("P01", "P02", "P03", "P11", "P12", "P13", "O00", "O10",),
    ("P21", "P22", "P23", "W0", "O01", "W1", "O11", "O20",),
    ("P31", "Y30", "X33", "P41", "Y40", "X43", "W2", "O21", "D33", "P32",),
    ("D43", "P42",),
    ("G41",),
    ("Z30", "G31", "Z31",),
    (),
    ("G32", "G33", "Z32", "Z33", "R30",),
    ("R31", "R32", "R33",),
    ("G42", "G43", "Z40", "Z41", "Z42", "Z43",),
    (),
    ("R40",),
    ("R41",),
    ("R42",),
    ("R43",),
)
INNER = (
    ("P01", "P02", "P03", "P11", "P12", "O10", "P13", "O00", "Q00", "Q10",),
    ("P21", "P22", "P23", "W0", "O01", "Q01", "W1", "O11", "Q11", "O20", "Q20",),
    ("P31", "Y30", "X33", "P41", "Y40", "X43", "N0", "N1", "M0", "M1", "W2", "F0", "O21", "F1", "Q21", "N2", "Z30",),
    ("M2", "G31", "Z31",),
    ("F2", "D33", "Z40", "P32", "G41", "Z41",),
    (),
    ("G32", "Z32", "G33", "Z33", "D43", "P42",),
    ("R30", "R31", "G42", "Z42", "G43", "Z43",),
    ("R32", "R33",),
    ("R40", "R41",),
    ("R42", "R43",),
    (),
    (),
    (),
    (),
)


def rows_at(start, size):
    return pl.ds(pl.multiple_of(start, 128), size)


def layer_kernel(
    ng,
    tok, mixg, gv, gg, taps, chg, mo, mlpg, up, dn,
    out,
    fgv, fgg, fmo, fup, fdn, stage_up, stage_dn,
    nrm, pad, phase, cv, hid, st, st_all,
    acc, resid, nm_all, act, fin,
    sbo1, sbi1, rdo1, rdi1, sbo2, sbi2, rdo2, rdi2,
    ws, wr, lsem, tsem, nsem, ssem, rsem, dsem, fsem,
):
    f, t = lax.axis_index("fs"), lax.axis_index("tp")
    x, y = lax.rem(f, 2), lax.rem(lax.div(f, 2), 2)
    zp, zh = lax.rem(lax.div(f, 4), 2), lax.div(f, 8)
    mid = lax.rem(zp + zh, 2)
    sib = 1 - t
    L = tok.shape[0] // 2
    half = ng * L
    width = tok.shape[1]
    chans = fgv.shape[1]
    hidden = fup.shape[1]
    depth = gv.shape[0]
    sends = []

    def flip(coord, bit):
        return 1 - coord if bit else coord

    def chip(dq):
        return flip(mid, dq // 2) * 2 + flip(x, dq % 2)

    def fs_of(dq, do):
        return flip(zh, do // 2) * 8 + flip(zp, (dq // 2 + do // 2) % 2) * 4 + flip(y, do % 2) * 2 + flip(x, dq % 2)

    def seat(dq):
        return flip(y, dq // 2) * 2 + flip(x, dq % 2)

    def seat_fs(dq, do=0):
        return zh * 8 + zp * 4 + flip(y, dq // 2) * 2 + flip(x, dq % 2)

    p, s = chip(0), seat(0)
    near, mate = fs_of(2, 0), fs_of(0, 2)
    z = zh * 2 + zp
    z_near = zh * 2 + 1 - zp
    z_mate, z_far = (1 - zh) * 2 + zh, (1 - zh) * 2 + 1 - zh
    outer, inner = mid == 0, mid == 1

    def remote(src, dst, s_sem, r_sem, device):
        return pltpu.make_async_remote_copy(
            src_ref=src, dst_ref=dst, send_sem=s_sem, recv_sem=r_sem,
            device_id=device, device_id_type=MESH,
        )

    def push(*args):
        copy = remote(*args)
        copy.start()
        sends.append(copy)

    def arrived(dst, s_sem, r_sem):
        remote(dst, dst, s_sem, r_sem, (f, sib)).wait_recv()

    barrier = pltpu.get_barrier_semaphore()
    peers = [(seat_fs(dq), u) for dq in range(1, ng) for u in (t, sib)]
    peers += [(f, sib), (near, t), (fs_of(3, 0), t), (mate, t)]
    for peer in peers:
        pl.semaphore_signal(barrier, inc=1, device_id=peer, device_id_type=MESH)

    weights = (
        (lambda q: gv.at[:, rows_at(q * chans, chans)], lambda g: fgv.at[rows_at(g * depth, depth), :]),
        (lambda q: gg.at[:, rows_at(q * chans, chans)], lambda g: fgg.at[rows_at(g * depth, depth), :]),
        (lambda q: mo.at[rows_at(q * chans, chans), :], lambda g: fmo.at[:, rows_at(g * depth, depth)]),
        (lambda q: up.at[:, rows_at(q * hidden, hidden)], lambda g: fup.at[rows_at(g * depth, depth), :]),
        (lambda q: dn.at[rows_at(q * hidden, hidden), :], lambda g: fdn.at[:, rows_at(g * depth, depth)]),
    )

    stage = (stage_up, stage_dn)

    def parts(op):
        kind, a, dq = op[0], int(op[1]), int((op + "0")[2])
        src, dst = weights[a]
        part, place = (seat, seat_fs) if a < 3 else (chip, fs_of)

        def mk(s_at, r_at, piece, to, own=None):
            return remote(piece if own is None else own, piece, ws.at[a, s_at], wr.at[a, r_at], (to, t))

        if kind == "P":
            return [], [mk(dq, dq, dst(f), place(dq, 0), src(part(dq)))]
        if kind == "X":
            return [], [mk(0, 0, stage[a - 3], fs_of(1, 0), src(chip(3)))]
        if kind == "D":
            return [mk(0, 0, stage[a - 3], f)], [mk(3, 3, dst(fs_of(1, 0)), near, stage[a - 3])]
        if kind == "W":
            return [mk(0, i, dst(place(i, 0)), f) for i in (1, 2, 3)], []
        if kind in "YGZ":
            do = 2 if kind == "Z" else 1
            piece = dst(fs_of(dq, 0))
            come = [mk(0, dq, piece, f)] if kind == "G" else []
            k = do * ng + dq
            return come, [mk(k, k, piece, fs_of(0, do), src(p) if dq == 0 else None)]
        if kind == "R":
            piece = dst(fs_of(dq, 2))
            k = 3 * ng + dq
            return [mk(0, 2 * ng + dq, piece, f)], [mk(k, k, piece, fs_of(0, 1))]
        plane = planes[a]
        if kind in "OQ":
            k, to = (4, near) if kind == "O" else (8, mate)
            own = src(part(0))
            return [], [mk(k + i, k + i, dst(place(i, 0)), to, None if i else own) for i in ((1, 2, 3) if dq else (0,))]
        if kind == "N":
            return [mk(0, 4 + i, dst(line_fs(z_near, i)), f) for i in range(4)], [mk(12, 12, plane(z_near), mate)]
        if kind == "M":
            return [mk(0, 8 + i, dst(line_fs(z_mate, i)), f) for i in range(4)], [mk(13, 13, plane(z_mate), near)]
        return [mk(0, 12, plane(z_far), f)], [mk(14, 14, plane(z_far), near)]

    def run(ops):
        for op in ops:
            come, go = parts(op)
            for copy in come:
                copy.wait_recv()
            if op[0] == "W":
                local(int(op[1])).wait()
            for copy in go:
                copy.start()

    def drain(plan):
        for ops in plan:
            for op in ops:
                for copy in parts(op)[1]:
                    copy.wait_send()

    def gap(i):
        if OUTER[i] == INNER[i]:
            run(OUTER[i])
            return
        for plan, when in ((OUTER, outer), (INNER, inner)):
            if plan[i]:
                pl.when(when)(functools.partial(run, plan[i]))

    def whole(a):
        dst = weights[a][1]
        for do in (1, 3):
            for dq in range(ng):
                arrived(dst(fs_of(dq, do)), ws.at[a, 0], wr.at[a, do * ng + dq])
        local(a).wait()

    def local(a):
        src, dst = weights[a]
        return pltpu.make_async_copy(src(s if a < 3 else p), dst(f), lsem.at[a])

    planes = (
        lambda g: fgv.at[rows_at(g * ng * depth, ng * depth), :],
        lambda g: fgg.at[rows_at(g * ng * depth, ng * depth), :],
        lambda g: fmo.at[:, rows_at(g * ng * depth, ng * depth)],
    )

    def line_fs(g, i):
        return g * ng + seat(i)

    def line_whole(a):
        for i in range(ng):
            arrived(weights[a][1](line_fs(z_near, i)), ws.at[a, 0], wr.at[a, 4 + i])
        for g, r_at in ((z_mate, 13), (z_far, 14)):
            arrived(planes[a](g), ws.at[a, 0], wr.at[a, r_at])

    first = (nrm, tsem, seat, seat_fs)
    second = (nm_all, nsem, chip, fs_of)

    def gather_start(buf, sem, part, place):
        own = buf.at[rows_at(t * half + part(0) * L, L)]
        for dq in (2, 1):
            push(own, own, sem.at[0, dq], sem.at[1, dq], (place(dq, 0), t))
        push(own, own, sem.at[2, 0], sem.at[3, 0], (f, sib))

    def gather_relay(rows, *which):
        buf, sem, part, place = rows
        for dq in which:
            block = buf.at[rows_at(t * half + part(dq) * L, L)]
            arrived(block, sem.at[0, 0], sem.at[1, dq])
            if dq == 2:
                push(block, block, sem.at[0, 3], sem.at[1, 3], (place(1, 0), t))
            push(block, block, sem.at[2, dq], sem.at[3, dq], (f, sib))

    def gather_finish(rows, *which):
        buf, sem, part, place = rows
        for dq in which:
            arrived(buf.at[rows_at(sib * half + part(dq) * L, L)], sem.at[0, 0], sem.at[3, dq])

    step = 16

    def norm_rows(load, gain, dst, start):
        def body(i, _):
            value = load(i * step).astype(F32)
            scale = lax.rsqrt(jnp.mean(value * value, axis=-1, keepdims=True) + norm_floor)
            dst[pl.ds(pl.multiple_of(start + i * step, step), step), :] = (
                value * scale * gain[...]
            ).astype(BF16)
            return 0

        lax.fori_loop(0, L // step, body, 0)

    def from_ref(ref, base):
        return lambda i: ref[pl.ds(pl.multiple_of(base + i, step), step), :]

    norm_rows(from_ref(tok, t * L), mixg, nrm, t * half + s * L)
    pl.semaphore_wait(barrier, len(peers))
    gap(0)
    for a in range(5):
        local(a).start()
    gather_start(*first)
    gap(1)
    gather_relay(first, 2, 1)
    gap(2)
    gather_finish(first, 0, 1)

    @pl.when(outer)
    def _():
        line_whole(0)
        line_whole(1)

    pad[...] = jnp.zeros_like(pad)
    st[...] = jnp.zeros_like(st)
    taps_n = taps.shape[0]
    reach = taps_n // 2
    lead = (reach + 7) // 8 * 8
    reach_lead = lead - reach
    own_cols = s * chans
    eye = lax.broadcasted_iota(jnp.int32, (L, L), 0) == lax.broadcasted_iota(jnp.int32, (L, L), 1)

    def conv_half(pair_base):
        def glu_rows(u, _):
            rows = rows_at(u * half + pair_base * L, 2 * L)
            left = nrm[rows, :]
            values = jnp.dot(left, fgv[...], preferred_element_type=F32)
            gating = jnp.dot(left, fgg[...], preferred_element_type=F32)
            cv[rows, :] = (values * jax.nn.sigmoid(gating)).astype(BF16).astype(F32)
            return 0

        def conv_block(i, _):
            b = lax.rem(i, 2) * ng + pair_base + lax.div(i, 2)
            rows = rows_at(b * L, L)
            sums = jnp.zeros((L, 1), F32)
            squares = jnp.zeros((L, 1), F32)
            for c in range(chans // 128):
                at = pl.ds(c * 128, 128)
                pad[pl.ds(lead, L), :] = cv[rows, at]
                window = pad[...]
                for r in range(8):
                    partial = jnp.zeros((L + 8, 128), F32)
                    for m in range(lead // 4):
                        j = 8 * m + r - reach_lead
                        if 0 <= j < taps_n:
                            tap = taps[pl.ds(j, 1), rows_at(own_cols + c * 128, 128)]
                            partial = partial + window[8 * m : 8 * m + L + 8] * tap
                    phase[r] = partial
                total = phase[0, pl.ds(0, L), :]
                for r in range(1, 8):
                    total = total + phase[r, pl.ds(r, L), :]
                cv[rows, at] = total
                sums = sums + jnp.sum(total, axis=1, keepdims=True)
                squares = squares + jnp.sum(total * total, axis=1, keepdims=True)
            st[b, pl.ds(0, 1), :] = jnp.sum(jnp.where(eye, sums, 0.0), axis=0, keepdims=True)
            st[b, pl.ds(1, 1), :] = jnp.sum(jnp.where(eye, squares, 0.0), axis=0, keepdims=True)
            return 0

        lax.fori_loop(0, 2, glu_rows, 0)
        lax.fori_loop(0, ng, conv_block, 0)

    conv_half(y * 2)
    gather_relay(first, 3)
    gap(3)
    gather_finish(first, 2, 3)
    conv_half((1 - y) * 2)

    slots = [(dq, du) for dq in range(ng) for du in range(2) if (dq, du) != (0, 0)]
    for dq, du in slots:
        push(
            st, st_all.at[dq * 2 + du],
            ssem.at[0, dq * 2 + du], ssem.at[1, dq * 2 + du],
            (seat_fs(dq), t if du == 0 else sib),
        )
    gap(4)
    for dq, du in slots:
        arrived(st_all.at[dq * 2 + du], ssem.at[0, 0], ssem.at[1, dq * 2 + du])

    def hidden_block(b, _):
        rows = rows_at(b * L, L)
        total = st[b]
        for dq, du in slots:
            total = total + st_all[dq * 2 + du, b]
        count = chans * ng * 2
        sums = jnp.sum(jnp.where(eye, total[0:1, :], 0.0), axis=1, keepdims=True)
        squares = jnp.sum(jnp.where(eye, total[1:2, :], 0.0), axis=1, keepdims=True)
        centre = sums / count
        spread = squares / count - centre * centre
        value = (cv[rows, :] - centre) * lax.rsqrt(spread + norm_floor)
        value = value * chg[:, rows_at(own_cols, chans)]
        hid[rows, :] = (value * jax.nn.sigmoid(value)).astype(BF16)
        return 0

    lax.fori_loop(0, 2 * ng, hidden_block, 0)

    cols = 512
    span = 32
    chunks = [pl.ds(n * cols, cols) for n in range(width // cols)]

    def over_rows(body):
        def go(i, _):
            body(pl.multiple_of(i * span, span))
            return 0

        lax.fori_loop(0, L // span, go, 0)

    def mix_partial(n, dq):
        at, base = chunks[n], seat(dq) * L

        def add(i):
            row = pl.ds(pl.multiple_of(base + i, span), span)
            total = acc[row, at] + sbi1[row, at].astype(F32)
            if dq == 2:
                total = total + rdi1[2, pl.ds(i, span), at].astype(F32)
            rdo1[row, at] = total.astype(BF16)

        over_rows(add)
        push(
            rdo1.at[rows_at(base, L), at], rdi1.at[dq - 1, :, at],
            rsem.at[0, dq, n], rsem.at[1, dq, n], (seat_fs(2 if dq == 2 else 1), t),
        )

    def reduce_mixed():
        for n, at in enumerate(chunks):
            sbo1[:, at] = jnp.dot(
                hid[rows_at(sib * half, half), :], fmo[:, at], preferred_element_type=F32
            ).astype(BF16)
            push(sbo1.at[:, at], sbi1.at[:, at], rsem.at[0, 0, n], rsem.at[1, 0, n], (f, sib))

        def mine(n, _):
            at = rows_at(n * cols, cols)
            acc[:, at] = jnp.dot(
                hid[rows_at(t * half, half), :], fmo[:, at], preferred_element_type=F32
            )
            return 0

        lax.fori_loop(0, width // cols, mine, 0)
        for dq in (3, 1):
            for n, at in enumerate(chunks):
                if dq == 3:
                    arrived(sbi1.at[:, at], rsem.at[0, 0, 0], rsem.at[1, 0, n])
                mix_partial(n, dq)
        gap(6)
        for n, at in enumerate(chunks):
            arrived(rdi1.at[2, :, at], rsem.at[0, 0, 0], rsem.at[1, 3, n])
            mix_partial(n, 2)

    def reduced(i):
        at = pl.ds(pl.multiple_of(s * L + i * step, step), step)
        total = acc[at, :] + sbi1[at, :].astype(F32)
        for dq in (1, 2):
            total = total + rdi1[dq - 1, pl.ds(pl.multiple_of(i * step, step), step), :].astype(F32)
        return total.astype(BF16).astype(F32)

    @pl.when(outer)
    def _():
        line_whole(2)

    gap(5)
    reduce_mixed()
    gap(7)
    for dq in (1, 2):
        for n, at in enumerate(chunks):
            arrived(rdi1.at[dq - 1, :, at], rsem.at[0, 0, 0], rsem.at[1, dq, n])

    def resid_rows(i, _):
        at = pl.ds(pl.multiple_of(i * step, step), step)
        own = tok[pl.ds(pl.multiple_of(t * L + i * step, step), step), :].astype(F32)
        value = own + reduced(i)
        resid[at, :] = value
        scale = lax.rsqrt(jnp.mean(value * value, axis=-1, keepdims=True) + norm_floor)
        nm_all[pl.ds(pl.multiple_of(t * half + p * L + i * step, step), step), :] = (
            value * scale * mlpg[...]
        ).astype(BF16)
        return 0

    lax.fori_loop(0, L // step, resid_rows, 0)
    gather_start(*second)
    gap(8)
    gather_relay(second, 2)
    gap(9)
    gather_relay(second, 1, 3)
    gap(10)
    whole(3)

    def up_half(u):
        def body(n, _):
            at = rows_at(n * 256, 256)
            value = jnp.dot(
                nm_all[rows_at(u * half, half), :], fup[:, at], preferred_element_type=F32
            )
            value = jnp.maximum(value, 0.0)
            act[rows_at(u * half, half), at] = (value * value).astype(BF16)
            return 0

        lax.fori_loop(0, hidden // 256, body, 0)

    gap(11)
    up_half(t)
    gap(12)
    gather_finish(second, 0, 1, 2, 3)
    up_half(sib)

    pair = 2 * depth
    def pair_at(g, j):
        return rows_at((flip(zh, g // 2) * 8 + j * 4 + flip(y, g % 2) * 2) * depth, pair)

    def down_group(g):
        def theirs(j, _):
            at = pair_at(g, j)
            sbo2[:, at] = jnp.dot(
                act[rows_at(sib * half, half), :], fdn[:, at], preferred_element_type=F32
            ).astype(BF16)
            return 0

        def mine(j, _):
            at = pair_at(g, j)
            acc[:, at] = jnp.dot(
                act[rows_at(t * half, half), :], fdn[:, at], preferred_element_type=F32
            )
            return 0

        lax.fori_loop(0, 2, theirs, 0)
        for j in range(2):
            at = pair_at(g, j)
            push(sbo2.at[:, at], sbi2.at[:, at], dsem.at[0, g * 2 + j, 0], dsem.at[1, g * 2 + j, 0], (f, sib))
        lax.fori_loop(0, 2, mine, 0)
        for j in range(2):
            arrived(sbi2.at[:, pair_at(g, j)], dsem.at[0, 0, 0], dsem.at[1, g * 2 + j, 0])
        for dq in (3, 1):
            for j in range(2):
                pass_partial(g, j, dq)

    def pass_partial(g, j, dq):
        at, base = pair_at(g, j), chip(dq) * L

        def add(i):
            row = pl.ds(pl.multiple_of(base + i, span), span)
            total = acc[row, at] + sbi2[row, at].astype(F32)
            if dq == 2:
                total = total + rdi2[2, pl.ds(i, span), at].astype(F32)
            rdo2[row, at] = total.astype(BF16)

        over_rows(add)
        push(
            rdo2.at[rows_at(base, L), at], rdi2.at[dq - 1, :, at],
            dsem.at[0, g * 2 + j, dq], dsem.at[1, g * 2 + j, dq], (fs_of(2 if dq == 2 else 1, 0), t),
        )

    def down_near(g):
        for j in range(2):
            arrived(rdi2.at[2, :, pair_at(g, j)], dsem.at[0, 0, 0], dsem.at[1, g * 2 + j, 3])
            pass_partial(g, j, 2)

    def down_final(g):
        for j in range(2):
            at = pair_at(g, j)
            for dq in (1, 2):
                arrived(rdi2.at[dq - 1, :, at], dsem.at[0, 0, 0], dsem.at[1, g * 2 + j, dq])

            def finish(i):
                row = pl.ds(pl.multiple_of(p * L + i, span), span)
                here = pl.ds(i, span)
                total = acc[row, at] + sbi2[row, at].astype(F32)
                total = total + rdi2[0, here, at].astype(F32) + rdi2[1, here, at].astype(F32)
                value = (resid[here, at] + total.astype(BF16).astype(F32)).astype(BF16)
                fin[0, here, at] = value
                out[pl.ds(pl.multiple_of(t * L + i, span), span), at] = value

            over_rows(finish)
            push(fin.at[0, :, at], fin.at[1, :, at], fsem.at[0, g * 2 + j], fsem.at[1, g * 2 + j], (f, sib))

    def down_copy(g):
        for j in range(2):
            at = pair_at(g, j)
            arrived(fin.at[1, :, at], fsem.at[0, 0], fsem.at[1, g * 2 + j])
            out[rows_at(sib * L, L), at] = fin[1, :, at]

    def down_wait(do):
        for dq in range(ng):
            arrived(weights[4][1](fs_of(dq, do)), ws.at[4, 0], wr.at[4, do * ng + dq])

    local(4).wait()
    gap(13)
    down_group(0)
    gap(14)
    down_wait(1)
    down_group(1)
    down_near(0)
    down_group(2)
    down_near(1)
    down_final(0)
    down_wait(3)
    down_group(3)
    down_near(2)
    down_final(1)
    down_copy(0)
    down_near(3)
    down_final(2)
    down_copy(1)
    down_final(3)
    down_copy(2)
    down_copy(3)
    for copy in sends:
        copy.wait_send()
    for plan, when in ((OUTER, outer), (INNER, inner)):
        pl.when(when)(functools.partial(drain, plan))


def fused_device(ng, nz, tokens, mix_gain, glu_value, glu_gate, conv_taps, chan_gain, mix_out, mlp_gain, up_weight, down_weight):
    rows, width = tokens.shape
    fs = ng * nz
    L = rows // 2
    half = ng * L
    chans = glu_value.shape[1] // ng
    hidden = up_weight.shape[1] // ng
    depth = glu_value.shape[0]
    blocks = 2 * ng
    vm = pltpu.VMEM
    dma = pltpu.SemaphoreType.DMA
    reduce_bufs = [
        vm((half, width), BF16), vm((half, width), BF16), vm((half, width), BF16),
        vm((ng - 1, L, width), BF16),
    ]
    scratch = [
        vm((fs * depth, chans), BF16), vm((fs * depth, chans), BF16), vm((chans, width), BF16),
        vm((fs * depth, hidden), BF16), vm((hidden, width), BF16),
        vm((depth, hidden), BF16), vm((hidden, depth), BF16),
        vm((2 * half, width), BF16),
        vm((L + 32, 128), F32), vm((8, L + 8, 128), F32), vm((2 * half, chans), F32), vm((2 * half, chans), BF16),
        vm((blocks, 8, L), F32), vm((blocks, blocks, 8, L), F32),
        vm((half, width), F32), vm((L, width), F32), vm((2 * half, width), BF16),
        vm((2 * half, hidden), BF16), vm((2, L, width), BF16),
        *reduce_bufs, *reduce_bufs,
        dma((5, fs)), dma((5, fs)), dma((5,)), dma((4, ng)), dma((4, ng)),
        dma((2, blocks)), dma((2, ng, 4)), dma((2, 2 * ng, 4)), dma((2, 2 * ng)),
    ]
    return pl.pallas_call(
        functools.partial(layer_kernel, ng),
        out_shape=jax.ShapeDtypeStruct((rows, width), BF16),
        in_specs=[pl.BlockSpec(memory_space=vm)] * 10,
        out_specs=pl.BlockSpec(memory_space=vm),
        scratch_shapes=scratch,
        compiler_params=pltpu.CompilerParams(
            collective_id=0, has_side_effects=True, vmem_limit_bytes=60 * 1024 * 1024
        ),
    )(
        tokens, mix_gain[None], glu_value, glu_gate, conv_taps, chan_gain[None], mix_out,
        mlp_gain[None], up_weight, down_weight,
    )


def per_device(*args):
    tokens, glu_value, conv_taps = args[0], args[2], args[4]
    fs, tp = lax.axis_size("fs"), lax.axis_size("tp")
    group = 4
    fits = (
        tp == 2
        and fs == group * 4
        and tokens.shape[0] == 2 * LEN
        and glu_value.shape[0] % 128 == 0
        and conv_taps.shape[1] % (group * 128) == 0
        and conv_taps.shape[0] <= 31
    )
    if fits:
        return fused_device(group, fs // group, *args)
    return plain_device(*args)


def solution(mesh):
    in_specs = (
        P("fs", None),
        P(),
        P("fs", "tp"),
        P("fs", "tp"),
        P(None, "tp"),
        P("tp"),
        P("tp", "fs"),
        P(),
        P("fs", "tp"),
        P("tp", "fs"),
    )
    out_specs = P("fs", None)
    return jax.shard_map(
        per_device, mesh=mesh, in_specs=in_specs, out_specs=out_specs, check_vma=False
    )
```

```python
import functools

import jax
import jax.numpy as jnp
from jax import lax
from jax.experimental import pallas as pl
from jax.experimental.pallas import tpu as pltpu
from jax.sharding import PartitionSpec as P

C = 2048
LEN = 128


norm_floor = 0.05


def rms_scale(stream, gain):
    return stream * lax.rsqrt(jnp.mean(stream * stream, axis=-1, keepdims=True) + norm_floor) * gain


def bf16_round(value):
    return lax.optimization_barrier(value.astype(jnp.bfloat16)).astype(jnp.float32)


def depthwise(glu, conv_taps):
    seqs = glu.shape[0] // LEN
    blocks = glu.reshape(seqs, LEN, glu.shape[1]).astype(jnp.float32)
    reach = conv_taps.shape[0] // 2
    padded = jnp.pad(blocks, ((0, 0), (reach, reach), (0, 0)))
    total = jnp.zeros_like(blocks)
    for offset in range(conv_taps.shape[0]):
        total = total + padded[:, offset : offset + LEN] * conv_taps[offset]
    return total.reshape(glu.shape)


def swap_then_gather(weight, inner, outer, split, join):
    own = lax.all_to_all(
        weight, "fs", split_axis=split, concat_axis=join, axis_index_groups=inner, tiled=True
    )
    return lax.all_gather(own, "fs", axis=join, axis_index_groups=outer, tiled=True)


def shared_sum(partial, inner, tp):
    part = lax.all_to_all(
        partial, "fs", split_axis=0, concat_axis=0, axis_index_groups=inner, tiled=True
    )
    group = len(inner[0])
    rows = partial.shape[0] // group
    part = part.reshape(group, tp, rows // tp, -1).transpose(1, 0, 2, 3)
    part = lax.all_to_all(part, "tp", split_axis=0, concat_axis=0, tiled=True)
    return bf16_round(jnp.sum(part.astype(jnp.float32), axis=(0, 1)))


def plain_device(
    tokens,
    mix_gain,
    glu_value,
    glu_gate,
    conv_taps,
    chan_gain,
    mix_out,
    mlp_gain,
    up_weight,
    down_weight,
):
    fs, tp = lax.axis_size("fs"), lax.axis_size("tp")
    group = 4 if fs % 4 == 0 else 1
    inner = [[o * group + i for i in range(group)] for o in range(fs // group)]
    outer = [[o * group + i for o in range(fs // group)] for i in range(group)]
    place = lax.rem(lax.axis_index("fs"), group)

    value_w = swap_then_gather(glu_value, inner, outer, 1, 0)
    gate_w = swap_then_gather(glu_gate, inner, outer, 1, 0)
    mix_w = swap_then_gather(mix_out, inner, outer, 0, 1)
    up_w = swap_then_gather(up_weight, inner, outer, 1, 0)
    down_w = swap_then_gather(down_weight, inner, outer, 0, 1)

    stream = tokens.astype(jnp.float32)
    normed = rms_scale(stream, mix_gain).astype(jnp.bfloat16)
    normed = lax.all_gather(normed, "fs", axis=0, axis_index_groups=inner, tiled=True)
    values = jnp.dot(normed, value_w, preferred_element_type=jnp.float32)
    gating = jnp.dot(normed, gate_w, preferred_element_type=jnp.float32)
    glu = (values * jax.nn.sigmoid(gating)).astype(jnp.bfloat16)
    channels = value_w.shape[1]
    taps = lax.dynamic_slice_in_dim(conv_taps, place * channels, channels, 1)
    gain = lax.dynamic_slice_in_dim(chan_gain, place * channels, channels, 0)
    convolved = depthwise(glu, taps)
    both = jnp.stack(
        (jnp.sum(convolved, axis=-1), jnp.sum(convolved * convolved, axis=-1))
    )
    both = jnp.sum(lax.all_gather(both, "fs", axis=0, axis_index_groups=inner), axis=0)
    both = lax.psum(both, "tp")
    centre = (both[0] / C)[:, None]
    spread = (both[1] / C)[:, None] - centre * centre
    hidden = jax.nn.silu((convolved - centre) * lax.rsqrt(spread + norm_floor) * gain).astype(
        jnp.bfloat16
    )
    mixed = shared_sum(
        jnp.dot(hidden, mix_w, preferred_element_type=jnp.float32).astype(jnp.bfloat16), inner, tp
    )
    own_rows = stream.shape[0] // tp
    own_stream = lax.dynamic_slice_in_dim(stream, lax.axis_index("tp") * own_rows, own_rows, 0)
    resid = own_stream + mixed
    normed_mlp = rms_scale(resid, mlp_gain).astype(jnp.bfloat16)
    normed_mlp = lax.all_gather(normed_mlp, "fs", axis=0, axis_index_groups=inner)
    normed_mlp = lax.all_gather(normed_mlp, "tp", axis=1).reshape(-1, normed.shape[1])
    active = jnp.square(
        jax.nn.relu(jnp.dot(normed_mlp, up_w, preferred_element_type=jnp.float32))
    ).astype(jnp.bfloat16)
    feed = shared_sum(
        jnp.dot(active, down_w, preferred_element_type=jnp.float32).astype(jnp.bfloat16), inner, tp
    )
    finished = (resid + feed).astype(jnp.bfloat16)
    return lax.all_gather(finished, "tp", axis=0, tiled=True)

MESH = pl.DeviceIdType.MESH
F32, BF16 = jnp.float32, jnp.bfloat16


OUTER = (
    ("P01", "P02", "P03", "P11", "P12", "P13", "O00", "O10", "P32",),
    ("P21", "P22", "P23", "W0", "O01", "W1", "O11", "O20",),
    ("P31", "Y30", "X33", "P41", "Y40", "X43", "W2", "O21", "D33", "G31",),
    ("D43", "P42", "G41",),
    ("G32",),
    ("Z30", "Z31",),
    ("G33", "Z32", "Z33",),
    ("R30",),
    ("R31", "R32", "R33",),
    ("G42", "G43", "Z40", "Z41", "Z42", "Z43",),
    (),
    ("R40",),
    ("R41",),
    ("R42",),
    ("R43",),
)
INNER = (
    ("P01", "P02", "P03", "P11", "P12", "O10", "P13", "O00", "Q00", "Q10", "P32",),
    ("P21", "P22", "P23", "W0", "O01", "Q01", "W1", "O11", "Q11", "O20", "Q20",),
    ("P31", "Y30", "X33", "P41", "Y40", "X43", "N0", "N1", "M0", "M1", "W2", "F0", "O21", "F1", "Q21", "N2", "Z30",),
    ("M2", "G31", "Z31", "D33",),
    ("F2", "Z40", "G41", "Z41", "G32", "Z32",),
    (),
    ("G33", "Z33", "D43",),
    ("R30", "R31", "G42", "P42", "Z42", "G43", "Z43",),
    ("R32", "R33",),
    ("R40", "R41",),
    ("R42", "R43",),
    (),
    (),
    (),
    (),
)


def rows_at(start, size):
    return pl.ds(pl.multiple_of(start, 128), size)


def layer_kernel(
    ng,
    tok, mixg, gv_in, gg_in, taps, chg, mo_in, mlpg, up_in, dn_in,
    out,
    gv, gg, mo, up, dn, fgv, fgg, fmo, fup, fdn, stage_up, stage_dn,
    nrm, pad, phase, cv, hid, st, st_all,
    acc, resid, nm_all, act, fin,
    sbo1, sbi1, rdo1, rdi1, sbo2, sbi2, rdo2, rdi2,
    hsem, ws, wr, lsem, tsem, nsem, ssem, rsem, dsem, fsem,
):
    f, t = lax.axis_index("fs"), lax.axis_index("tp")
    x, y = lax.rem(f, 2), lax.rem(lax.div(f, 2), 2)
    zp, zh = lax.rem(lax.div(f, 4), 2), lax.div(f, 8)
    mid = lax.rem(zp + zh, 2)
    sib = 1 - t
    L = tok.shape[0] // 2
    half = ng * L
    width = tok.shape[1]
    chans = fgv.shape[1]
    hidden = fup.shape[1]
    depth = gv.shape[0]
    sends = []

    def flip(coord, bit):
        return 1 - coord if bit else coord

    def chip(dq):
        return flip(mid, dq // 2) * 2 + flip(x, dq % 2)

    def fs_of(dq, do):
        return flip(zh, do // 2) * 8 + flip(zp, (dq // 2 + do // 2) % 2) * 4 + flip(y, do % 2) * 2 + flip(x, dq % 2)

    def seat(dq):
        return flip(y, dq // 2) * 2 + flip(x, dq % 2)

    def seat_fs(dq, do=0):
        return zh * 8 + zp * 4 + flip(y, dq // 2) * 2 + flip(x, dq % 2)

    p, s = chip(0), seat(0)
    near, mate = fs_of(2, 0), fs_of(0, 2)
    z = zh * 2 + zp
    z_near = zh * 2 + 1 - zp
    z_mate, z_far = (1 - zh) * 2 + zh, (1 - zh) * 2 + 1 - zh
    outer, inner = mid == 0, mid == 1

    def remote(src, dst, s_sem, r_sem, device):
        return pltpu.make_async_remote_copy(
            src_ref=src, dst_ref=dst, send_sem=s_sem, recv_sem=r_sem,
            device_id=device, device_id_type=MESH,
        )

    def push(*args):
        copy = remote(*args)
        copy.start()
        sends.append(copy)

    def arrived(dst, s_sem, r_sem):
        remote(dst, dst, s_sem, r_sem, (f, sib)).wait_recv()

    loads = [
        pltpu.make_async_copy(src, dst, hsem.at[i])
        for i, (src, dst) in enumerate(((gv_in, gv), (gg_in, gg), (mo_in, mo), (up_in, up), (dn_in, dn)))
    ]
    for load in loads:
        load.start()
    barrier = pltpu.get_barrier_semaphore()
    peers = [(seat_fs(dq), u) for dq in range(1, ng) for u in (t, sib)]
    peers += [(f, sib), (near, t), (fs_of(3, 0), t), (mate, t)]
    for peer in peers:
        pl.semaphore_signal(barrier, inc=1, device_id=peer, device_id_type=MESH)

    weights = (
        (lambda q: gv.at[:, rows_at(q * chans, chans)], lambda g: fgv.at[rows_at(g * depth, depth), :]),
        (lambda q: gg.at[:, rows_at(q * chans, chans)], lambda g: fgg.at[rows_at(g * depth, depth), :]),
        (lambda q: mo.at[rows_at(q * chans, chans), :], lambda g: fmo.at[:, rows_at(g * depth, depth)]),
        (lambda q: up.at[:, rows_at(q * hidden, hidden)], lambda g: fup.at[rows_at(g * depth, depth), :]),
        (lambda q: dn.at[rows_at(q * hidden, hidden), :], lambda g: fdn.at[:, rows_at(g * depth, depth)]),
    )

    stage = (stage_up, stage_dn)

    def parts(op):
        kind, a, dq = op[0], int(op[1]), int((op + "0")[2])
        src, dst = weights[a]
        part, place = (seat, seat_fs) if a < 3 else (chip, fs_of)

        def mk(s_at, r_at, piece, to, own=None):
            return remote(piece if own is None else own, piece, ws.at[a, s_at], wr.at[a, r_at], (to, t))

        if kind == "P":
            return [], [mk(dq, dq, dst(f), place(dq, 0), src(part(dq)))]
        if kind == "X":
            return [], [mk(0, 0, stage[a - 3], fs_of(1, 0), src(chip(3)))]
        if kind == "D":
            return [mk(0, 0, stage[a - 3], f)], [mk(3, 3, dst(fs_of(1, 0)), near, stage[a - 3])]
        if kind == "W":
            return [mk(0, i, dst(place(i, 0)), f) for i in (1, 2, 3)], []
        if kind in "YGZ":
            do = 2 if kind == "Z" else 1
            piece = dst(fs_of(dq, 0))
            come = [mk(0, dq, piece, f)] if kind == "G" else []
            k = do * ng + dq
            return come, [mk(k, k, piece, fs_of(0, do), src(p) if dq == 0 else None)]
        if kind == "R":
            piece = dst(fs_of(dq, 2))
            k = 3 * ng + dq
            return [mk(0, 2 * ng + dq, piece, f)], [mk(k, k, piece, fs_of(0, 1))]
        plane = planes[a]
        if kind in "OQ":
            k, to = (4, near) if kind == "O" else (8, mate)
            own = src(part(0))
            return [], [mk(k + i, k + i, dst(place(i, 0)), to, None if i else own) for i in ((1, 2, 3) if dq else (0,))]
        if kind == "N":
            return [mk(0, 4 + i, dst(line_fs(z_near, i)), f) for i in range(4)], [mk(12, 12, plane(z_near), mate)]
        if kind == "M":
            return [mk(0, 8 + i, dst(line_fs(z_mate, i)), f) for i in range(4)], [mk(13, 13, plane(z_mate), near)]
        return [mk(0, 12, plane(z_far), f)], [mk(14, 14, plane(z_far), near)]

    def run(ops):
        for op in ops:
            come, go = parts(op)
            for copy in come:
                copy.wait_recv()
            if op[0] == "W":
                local(int(op[1])).wait()
            for copy in go:
                copy.start()

    def drain(plan):
        for ops in plan:
            for op in ops:
                for copy in parts(op)[1]:
                    copy.wait_send()

    def gap(i):
        if OUTER[i] == INNER[i]:
            run(OUTER[i])
            return
        for plan, when in ((OUTER, outer), (INNER, inner)):
            if plan[i]:
                pl.when(when)(functools.partial(run, plan[i]))

    def whole(a):
        dst = weights[a][1]
        for do in (1, 3):
            for dq in range(ng):
                arrived(dst(fs_of(dq, do)), ws.at[a, 0], wr.at[a, do * ng + dq])
        local(a).wait()

    def local(a):
        src, dst = weights[a]
        return pltpu.make_async_copy(src(s if a < 3 else p), dst(f), lsem.at[a])

    planes = (
        lambda g: fgv.at[rows_at(g * ng * depth, ng * depth), :],
        lambda g: fgg.at[rows_at(g * ng * depth, ng * depth), :],
        lambda g: fmo.at[:, rows_at(g * ng * depth, ng * depth)],
    )

    def line_fs(g, i):
        return g * ng + seat(i)

    def line_whole(a):
        for i in range(ng):
            arrived(weights[a][1](line_fs(z_near, i)), ws.at[a, 0], wr.at[a, 4 + i])
        for g, r_at in ((z_mate, 13), (z_far, 14)):
            arrived(planes[a](g), ws.at[a, 0], wr.at[a, r_at])

    first = (nrm, tsem, seat, seat_fs)
    second = (nm_all, nsem, chip, fs_of)

    def gather_start(buf, sem, part, place):
        own = buf.at[rows_at(t * half + part(0) * L, L)]
        for dq in (2, 1):
            push(own, own, sem.at[0, dq], sem.at[1, dq], (place(dq, 0), t))
        push(own, own, sem.at[2, 0], sem.at[3, 0], (f, sib))

    def gather_relay(rows, *which):
        buf, sem, part, place = rows
        for dq in which:
            block = buf.at[rows_at(t * half + part(dq) * L, L)]
            arrived(block, sem.at[0, 0], sem.at[1, dq])
            if dq == 2:
                push(block, block, sem.at[0, 3], sem.at[1, 3], (place(1, 0), t))
            push(block, block, sem.at[2, dq], sem.at[3, dq], (f, sib))

    def gather_finish(rows, *which):
        buf, sem, part, place = rows
        for dq in which:
            arrived(buf.at[rows_at(sib * half + part(dq) * L, L)], sem.at[0, 0], sem.at[3, dq])

    step = 16

    def norm_rows(load, gain, dst, start):
        def body(i, _):
            value = load(i * step).astype(F32)
            scale = lax.rsqrt(jnp.mean(value * value, axis=-1, keepdims=True) + norm_floor)
            dst[pl.ds(pl.multiple_of(start + i * step, step), step), :] = (
                value * scale * gain[...]
            ).astype(BF16)
            return 0

        lax.fori_loop(0, L // step, body, 0)

    def from_ref(ref, base):
        return lambda i: ref[pl.ds(pl.multiple_of(base + i, step), step), :]

    norm_rows(from_ref(tok, t * L), mixg, nrm, t * half + s * L)
    pl.semaphore_wait(barrier, len(peers))
    for load in loads:
        load.wait()
    gap(0)
    for a in range(5):
        local(a).start()
    gather_start(*first)
    gap(1)
    gather_relay(first, 2, 1)
    gap(2)
    gather_finish(first, 0, 1)

    @pl.when(outer)
    def _():
        line_whole(0)
        line_whole(1)

    pad[...] = jnp.zeros_like(pad)
    st[...] = jnp.zeros_like(st)
    taps_n = taps.shape[0]
    reach = taps_n // 2
    lead = (reach + 7) // 8 * 8
    reach_lead = lead - reach
    own_cols = s * chans
    eye = lax.broadcasted_iota(jnp.int32, (L, L), 0) == lax.broadcasted_iota(jnp.int32, (L, L), 1)

    def conv_half(pair_base):
        def glu_rows(u, _):
            rows = rows_at(u * half + pair_base * L, 2 * L)
            left = nrm[rows, :]
            values = jnp.dot(left, fgv[...], preferred_element_type=F32)
            gating = jnp.dot(left, fgg[...], preferred_element_type=F32)
            cv[rows, :] = (values * jax.nn.sigmoid(gating)).astype(BF16).astype(F32)
            return 0

        def conv_block(i, _):
            b = lax.rem(i, 2) * ng + pair_base + lax.div(i, 2)
            rows = rows_at(b * L, L)
            sums = jnp.zeros((L, 1), F32)
            squares = jnp.zeros((L, 1), F32)
            for c in range(chans // 128):
                at = pl.ds(c * 128, 128)
                pad[pl.ds(lead, L), :] = cv[rows, at]
                window = pad[...]
                for r in range(8):
                    partial = jnp.zeros((L + 8, 128), F32)
                    for m in range(lead // 4):
                        j = 8 * m + r - reach_lead
                        if 0 <= j < taps_n:
                            tap = taps[pl.ds(j, 1), rows_at(own_cols + c * 128, 128)]
                            partial = partial + window[8 * m : 8 * m + L + 8] * tap
                    phase[r] = partial
                total = phase[0, pl.ds(0, L), :]
                for r in range(1, 8):
                    total = total + phase[r, pl.ds(r, L), :]
                cv[rows, at] = total
                sums = sums + jnp.sum(total, axis=1, keepdims=True)
                squares = squares + jnp.sum(total * total, axis=1, keepdims=True)
            st[b, pl.ds(0, 1), :] = jnp.sum(jnp.where(eye, sums, 0.0), axis=0, keepdims=True)
            st[b, pl.ds(1, 1), :] = jnp.sum(jnp.where(eye, squares, 0.0), axis=0, keepdims=True)
            return 0

        lax.fori_loop(0, 2, glu_rows, 0)
        lax.fori_loop(0, ng, conv_block, 0)

    conv_half(y * 2)
    gather_relay(first, 3)
    gap(3)
    gather_finish(first, 2, 3)
    conv_half((1 - y) * 2)

    slots = [(dq, du) for dq in range(ng) for du in range(2) if (dq, du) != (0, 0)]
    for dq, du in slots:
        push(
            st, st_all.at[dq * 2 + du],
            ssem.at[0, dq * 2 + du], ssem.at[1, dq * 2 + du],
            (seat_fs(dq), t if du == 0 else sib),
        )
    gap(4)
    for dq, du in slots:
        arrived(st_all.at[dq * 2 + du], ssem.at[0, 0], ssem.at[1, dq * 2 + du])

    def hidden_block(b, _):
        rows = rows_at(b * L, L)
        total = st[b]
        for dq, du in slots:
            total = total + st_all[dq * 2 + du, b]
        count = chans * ng * 2
        sums = jnp.sum(jnp.where(eye, total[0:1, :], 0.0), axis=1, keepdims=True)
        squares = jnp.sum(jnp.where(eye, total[1:2, :], 0.0), axis=1, keepdims=True)
        centre = sums / count
        spread = squares / count - centre * centre
        value = (cv[rows, :] - centre) * lax.rsqrt(spread + norm_floor)
        value = value * chg[:, rows_at(own_cols, chans)]
        hid[rows, :] = (value * jax.nn.sigmoid(value)).astype(BF16)
        return 0

    lax.fori_loop(0, 2 * ng, hidden_block, 0)

    cols = 512
    span = 32
    chunks = [pl.ds(n * cols, cols) for n in range(width // cols)]

    def over_rows(body):
        def go(i, _):
            body(pl.multiple_of(i * span, span))
            return 0

        lax.fori_loop(0, L // span, go, 0)

    def mix_partial(n, dq):
        at, base = chunks[n], seat(dq) * L

        def add(i):
            row = pl.ds(pl.multiple_of(base + i, span), span)
            total = acc[row, at] + sbi1[row, at].astype(F32)
            if dq == 2:
                total = total + rdi1[2, pl.ds(i, span), at].astype(F32)
            rdo1[row, at] = total.astype(BF16)

        over_rows(add)
        push(
            rdo1.at[rows_at(base, L), at], rdi1.at[dq - 1, :, at],
            rsem.at[0, dq, n], rsem.at[1, dq, n], (seat_fs(2 if dq == 2 else 1), t),
        )

    def reduce_mixed():
        for n, at in enumerate(chunks):
            sbo1[:, at] = jnp.dot(
                hid[rows_at(sib * half, half), :], fmo[:, at], preferred_element_type=F32
            ).astype(BF16)
            push(sbo1.at[:, at], sbi1.at[:, at], rsem.at[0, 0, n], rsem.at[1, 0, n], (f, sib))

        def mine(n, _):
            at = rows_at(n * cols, cols)
            acc[:, at] = jnp.dot(
                hid[rows_at(t * half, half), :], fmo[:, at], preferred_element_type=F32
            )
            return 0

        lax.fori_loop(0, width // cols, mine, 0)
        for dq in (3, 1):
            for n, at in enumerate(chunks):
                if dq == 3:
                    arrived(sbi1.at[:, at], rsem.at[0, 0, 0], rsem.at[1, 0, n])
                mix_partial(n, dq)
        gap(6)
        for n, at in enumerate(chunks):
            arrived(rdi1.at[2, :, at], rsem.at[0, 0, 0], rsem.at[1, 3, n])
            mix_partial(n, 2)

    def reduced(i):
        at = pl.ds(pl.multiple_of(s * L + i * step, step), step)
        total = acc[at, :] + sbi1[at, :].astype(F32)
        for dq in (1, 2):
            total = total + rdi1[dq - 1, pl.ds(pl.multiple_of(i * step, step), step), :].astype(F32)
        return total.astype(BF16).astype(F32)

    @pl.when(outer)
    def _():
        line_whole(2)

    gap(5)
    reduce_mixed()
    gap(7)
    for dq in (1, 2):
        for n, at in enumerate(chunks):
            arrived(rdi1.at[dq - 1, :, at], rsem.at[0, 0, 0], rsem.at[1, dq, n])

    def resid_rows(i, _):
        at = pl.ds(pl.multiple_of(i * step, step), step)
        own = tok[pl.ds(pl.multiple_of(t * L + i * step, step), step), :].astype(F32)
        value = own + reduced(i)
        resid[at, :] = value
        scale = lax.rsqrt(jnp.mean(value * value, axis=-1, keepdims=True) + norm_floor)
        nm_all[pl.ds(pl.multiple_of(t * half + p * L + i * step, step), step), :] = (
            value * scale * mlpg[...]
        ).astype(BF16)
        return 0

    lax.fori_loop(0, L // step, resid_rows, 0)
    gather_start(*second)
    gap(8)
    gather_relay(second, 2)
    gap(9)
    gather_relay(second, 1, 3)
    gap(10)
    whole(3)

    def up_half(u):
        def body(n, _):
            at = rows_at(n * 256, 256)
            value = jnp.dot(
                nm_all[rows_at(u * half, half), :], fup[:, at], preferred_element_type=F32
            )
            value = jnp.maximum(value, 0.0)
            act[rows_at(u * half, half), at] = (value * value).astype(BF16)
            return 0

        lax.fori_loop(0, hidden // 256, body, 0)

    gap(11)
    up_half(t)
    gap(12)
    gather_finish(second, 0, 1, 2, 3)
    up_half(sib)

    pair = 2 * depth
    def pair_at(g, j):
        return rows_at((flip(zh, g // 2) * 8 + j * 4 + flip(y, g % 2) * 2) * depth, pair)

    def down_group(g):
        def theirs(j, _):
            at = pair_at(g, j)
            sbo2[:, at] = jnp.dot(
                act[rows_at(sib * half, half), :], fdn[:, at], preferred_element_type=F32
            ).astype(BF16)
            return 0

        def mine(j, _):
            at = pair_at(g, j)
            acc[:, at] = jnp.dot(
                act[rows_at(t * half, half), :], fdn[:, at], preferred_element_type=F32
            )
            return 0

        lax.fori_loop(0, 2, theirs, 0)
        for j in range(2):
            at = pair_at(g, j)
            push(sbo2.at[:, at], sbi2.at[:, at], dsem.at[0, g * 2 + j, 0], dsem.at[1, g * 2 + j, 0], (f, sib))
        lax.fori_loop(0, 2, mine, 0)
        for j in range(2):
            arrived(sbi2.at[:, pair_at(g, j)], dsem.at[0, 0, 0], dsem.at[1, g * 2 + j, 0])
        for dq in (3, 1):
            for j in range(2):
                pass_partial(g, j, dq)

    def pass_partial(g, j, dq):
        at, base = pair_at(g, j), chip(dq) * L

        def add(i):
            row = pl.ds(pl.multiple_of(base + i, span), span)
            total = acc[row, at] + sbi2[row, at].astype(F32)
            if dq == 2:
                total = total + rdi2[2, pl.ds(i, span), at].astype(F32)
            rdo2[row, at] = total.astype(BF16)

        over_rows(add)
        push(
            rdo2.at[rows_at(base, L), at], rdi2.at[dq - 1, :, at],
            dsem.at[0, g * 2 + j, dq], dsem.at[1, g * 2 + j, dq], (fs_of(2 if dq == 2 else 1, 0), t),
        )

    def down_near(g):
        for j in range(2):
            arrived(rdi2.at[2, :, pair_at(g, j)], dsem.at[0, 0, 0], dsem.at[1, g * 2 + j, 3])
            pass_partial(g, j, 2)

    def down_final(g):
        for j in range(2):
            at = pair_at(g, j)
            for dq in (1, 2):
                arrived(rdi2.at[dq - 1, :, at], dsem.at[0, 0, 0], dsem.at[1, g * 2 + j, dq])

            def finish(i):
                row = pl.ds(pl.multiple_of(p * L + i, span), span)
                here = pl.ds(i, span)
                total = acc[row, at] + sbi2[row, at].astype(F32)
                total = total + rdi2[0, here, at].astype(F32) + rdi2[1, here, at].astype(F32)
                value = (resid[here, at] + total.astype(BF16).astype(F32)).astype(BF16)
                fin[0, here, at] = value
                out[pl.ds(pl.multiple_of(t * L + i, span), span), at] = value

            over_rows(finish)
            push(fin.at[0, :, at], fin.at[1, :, at], fsem.at[0, g * 2 + j], fsem.at[1, g * 2 + j], (f, sib))

    def down_copy(g):
        for j in range(2):
            at = pair_at(g, j)
            arrived(fin.at[1, :, at], fsem.at[0, 0], fsem.at[1, g * 2 + j])
            out[rows_at(sib * L, L), at] = fin[1, :, at]

    def down_wait(do):
        for dq in range(ng):
            arrived(weights[4][1](fs_of(dq, do)), ws.at[4, 0], wr.at[4, do * ng + dq])

    local(4).wait()
    gap(13)
    down_group(0)
    gap(14)
    down_wait(1)
    down_group(1)
    down_near(0)
    down_group(2)
    down_near(1)
    down_final(0)
    down_wait(3)
    down_group(3)
    down_near(2)
    down_final(1)
    down_copy(0)
    down_near(3)
    down_final(2)
    down_copy(1)
    down_final(3)
    down_copy(2)
    down_copy(3)
    for copy in sends:
        copy.wait_send()
    for plan, when in ((OUTER, outer), (INNER, inner)):
        pl.when(when)(functools.partial(drain, plan))


def fused_device(ng, nz, tokens, mix_gain, glu_value, glu_gate, conv_taps, chan_gain, mix_out, mlp_gain, up_weight, down_weight):
    rows, width = tokens.shape
    fs = ng * nz
    L = rows // 2
    half = ng * L
    chans = glu_value.shape[1] // ng
    hidden = up_weight.shape[1] // ng
    depth = glu_value.shape[0]
    blocks = 2 * ng
    vm = pltpu.VMEM
    dma = pltpu.SemaphoreType.DMA
    reduce_bufs = [
        vm((half, width), BF16), vm((half, width), BF16), vm((half, width), BF16),
        vm((ng - 1, L, width), BF16),
    ]
    held = (2, 3, 6, 8, 9)
    scratch = [
        *(vm(w.shape, BF16) for w in (glu_value, glu_gate, mix_out, up_weight, down_weight)),
        vm((fs * depth, chans), BF16), vm((fs * depth, chans), BF16), vm((chans, width), BF16),
        vm((fs * depth, hidden), BF16), vm((hidden, width), BF16),
        vm((depth, hidden), BF16), vm((hidden, depth), BF16),
        vm((2 * half, width), BF16),
        vm((L + 32, 128), F32), vm((8, L + 8, 128), F32), vm((2 * half, chans), F32), vm((2 * half, chans), BF16),
        vm((blocks, 8, L), F32), vm((blocks, blocks, 8, L), F32),
        vm((half, width), F32), vm((L, width), F32), vm((2 * half, width), BF16),
        vm((2 * half, hidden), BF16), vm((2, L, width), BF16),
        *reduce_bufs, *reduce_bufs,
        dma((5,)), dma((5, fs)), dma((5, fs)), dma((5,)), dma((4, ng)), dma((4, ng)),
        dma((2, blocks)), dma((2, ng, 4)), dma((2, 2 * ng, 4)), dma((2, 2 * ng)),
    ]
    return pl.pallas_call(
        functools.partial(layer_kernel, ng),
        out_shape=jax.ShapeDtypeStruct((rows, width), BF16),
        in_specs=[pl.BlockSpec(memory_space=pl.ANY if i in held else vm) for i in range(10)],
        out_specs=pl.BlockSpec(memory_space=vm),
        scratch_shapes=scratch,
        compiler_params=pltpu.CompilerParams(
            collective_id=0, has_side_effects=True, vmem_limit_bytes=60 * 1024 * 1024
        ),
    )(
        tokens, mix_gain[None], glu_value, glu_gate, conv_taps, chan_gain[None], mix_out,
        mlp_gain[None], up_weight, down_weight,
    )


def per_device(*args):
    tokens, glu_value, conv_taps = args[0], args[2], args[4]
    fs, tp = lax.axis_size("fs"), lax.axis_size("tp")
    group = 4
    fits = (
        tp == 2
        and fs == group * 4
        and tokens.shape[0] == 2 * LEN
        and glu_value.shape[0] % 128 == 0
        and conv_taps.shape[1] % (group * 128) == 0
        and conv_taps.shape[0] <= 31
    )
    if fits:
        return fused_device(group, fs // group, *args)
    return plain_device(*args)


def solution(mesh):
    in_specs = (
        P("fs", None),
        P(),
        P("fs", "tp"),
        P("fs", "tp"),
        P(None, "tp"),
        P("tp"),
        P("tp", "fs"),
        P(),
        P("fs", "tp"),
        P("tp", "fs"),
    )
    out_specs = P("fs", None)
    return jax.shard_map(
        per_device, mesh=mesh, in_specs=in_specs, out_specs=out_specs, check_vma=False
    )
```

```python
import functools

import jax
import jax.numpy as jnp
from jax import lax
from jax.experimental import pallas as pl
from jax.experimental.pallas import tpu as pltpu
from jax.sharding import PartitionSpec as P

C = 2048
LEN = 128


norm_floor = 0.05


def rms_scale(stream, gain):
    return stream * lax.rsqrt(jnp.mean(stream * stream, axis=-1, keepdims=True) + norm_floor) * gain


def bf16_round(value):
    return lax.optimization_barrier(value.astype(jnp.bfloat16)).astype(jnp.float32)


def depthwise(glu, conv_taps):
    seqs = glu.shape[0] // LEN
    blocks = glu.reshape(seqs, LEN, glu.shape[1]).astype(jnp.float32)
    reach = conv_taps.shape[0] // 2
    padded = jnp.pad(blocks, ((0, 0), (reach, reach), (0, 0)))
    total = jnp.zeros_like(blocks)
    for offset in range(conv_taps.shape[0]):
        total = total + padded[:, offset : offset + LEN] * conv_taps[offset]
    return total.reshape(glu.shape)


def swap_then_gather(weight, inner, outer, split, join):
    own = lax.all_to_all(
        weight, "fs", split_axis=split, concat_axis=join, axis_index_groups=inner, tiled=True
    )
    return lax.all_gather(own, "fs", axis=join, axis_index_groups=outer, tiled=True)


def shared_sum(partial, inner, tp):
    part = lax.all_to_all(
        partial, "fs", split_axis=0, concat_axis=0, axis_index_groups=inner, tiled=True
    )
    group = len(inner[0])
    rows = partial.shape[0] // group
    part = part.reshape(group, tp, rows // tp, -1).transpose(1, 0, 2, 3)
    part = lax.all_to_all(part, "tp", split_axis=0, concat_axis=0, tiled=True)
    return bf16_round(jnp.sum(part.astype(jnp.float32), axis=(0, 1)))


def plain_device(
    tokens,
    mix_gain,
    glu_value,
    glu_gate,
    conv_taps,
    chan_gain,
    mix_out,
    mlp_gain,
    up_weight,
    down_weight,
):
    fs, tp = lax.axis_size("fs"), lax.axis_size("tp")
    group = 4 if fs % 4 == 0 else 1
    inner = [[o * group + i for i in range(group)] for o in range(fs // group)]
    outer = [[o * group + i for o in range(fs // group)] for i in range(group)]
    place = lax.rem(lax.axis_index("fs"), group)

    value_w = swap_then_gather(glu_value, inner, outer, 1, 0)
    gate_w = swap_then_gather(glu_gate, inner, outer, 1, 0)
    mix_w = swap_then_gather(mix_out, inner, outer, 0, 1)
    up_w = swap_then_gather(up_weight, inner, outer, 1, 0)
    down_w = swap_then_gather(down_weight, inner, outer, 0, 1)

    stream = tokens.astype(jnp.float32)
    normed = rms_scale(stream, mix_gain).astype(jnp.bfloat16)
    normed = lax.all_gather(normed, "fs", axis=0, axis_index_groups=inner, tiled=True)
    values = jnp.dot(normed, value_w, preferred_element_type=jnp.float32)
    gating = jnp.dot(normed, gate_w, preferred_element_type=jnp.float32)
    glu = (values * jax.nn.sigmoid(gating)).astype(jnp.bfloat16)
    channels = value_w.shape[1]
    taps = lax.dynamic_slice_in_dim(conv_taps, place * channels, channels, 1)
    gain = lax.dynamic_slice_in_dim(chan_gain, place * channels, channels, 0)
    convolved = depthwise(glu, taps)
    both = jnp.stack(
        (jnp.sum(convolved, axis=-1), jnp.sum(convolved * convolved, axis=-1))
    )
    both = jnp.sum(lax.all_gather(both, "fs", axis=0, axis_index_groups=inner), axis=0)
    both = lax.psum(both, "tp")
    centre = (both[0] / C)[:, None]
    spread = (both[1] / C)[:, None] - centre * centre
    hidden = jax.nn.silu((convolved - centre) * lax.rsqrt(spread + norm_floor) * gain).astype(
        jnp.bfloat16
    )
    mixed = shared_sum(
        jnp.dot(hidden, mix_w, preferred_element_type=jnp.float32).astype(jnp.bfloat16), inner, tp
    )
    own_rows = stream.shape[0] // tp
    own_stream = lax.dynamic_slice_in_dim(stream, lax.axis_index("tp") * own_rows, own_rows, 0)
    resid = own_stream + mixed
    normed_mlp = rms_scale(resid, mlp_gain).astype(jnp.bfloat16)
    normed_mlp = lax.all_gather(normed_mlp, "fs", axis=0, axis_index_groups=inner)
    normed_mlp = lax.all_gather(normed_mlp, "tp", axis=1).reshape(-1, normed.shape[1])
    active = jnp.square(
        jax.nn.relu(jnp.dot(normed_mlp, up_w, preferred_element_type=jnp.float32))
    ).astype(jnp.bfloat16)
    feed = shared_sum(
        jnp.dot(active, down_w, preferred_element_type=jnp.float32).astype(jnp.bfloat16), inner, tp
    )
    finished = (resid + feed).astype(jnp.bfloat16)
    return lax.all_gather(finished, "tp", axis=0, tiled=True)

MESH = pl.DeviceIdType.MESH
F32, BF16 = jnp.float32, jnp.bfloat16


OUTER = (
    ("P01", "P02", "P03", "P11", "P12", "P13", "O00", "O10", "P32",),
    ("P21", "P22", "P23", "W0", "O01", "W1", "O11", "O20",),
    ("P31", "Y30", "X33", "P41", "Y40", "X43", "W2", "O21", "D33", "G31",),
    ("G32", "D43", "P42", "G41",),
    (),
    ("Z30", "Z31",),
    ("G33", "Z32", "Z33",),
    ("R30",),
    ("R31", "R32", "R33",),
    ("G42", "G43", "Z40", "Z41", "Z42", "Z43",),
    (),
    ("R40",),
    ("R41",),
    ("R42",),
    ("R43",),
)
INNER = (
    ("P01", "P02", "P03", "P11", "P12", "O10", "P13", "O00", "Q00", "Q10", "P32",),
    ("P21", "P22", "P23", "W0", "O01", "Q01", "W1", "O11", "Q11", "O20", "Q20",),
    ("P31", "Y30", "X33", "P41", "Y40", "X43", "N0", "N1", "M0", "M1", "W2", "F0", "O21", "F1", "Q21", "N2", "Z30",),
    ("M2", "G31", "Z31", "D33",),
    ("F2", "Z40", "G41", "Z41", "G32", "Z32",),
    (),
    ("G33", "Z33", "D43",),
    ("R30", "R31", "G42", "P42", "Z42", "G43", "Z43",),
    ("R32", "R33",),
    ("R40", "R41",),
    ("R42", "R43",),
    (),
    (),
    (),
    (),
)


def rows_at(start, size):
    return pl.ds(pl.multiple_of(start, 128), size)


def layer_kernel(
    ng,
    tok, mixg, gv_in, gg_in, taps, chg, mo_in, mlpg, up_in, dn_in,
    out,
    gv, gg, mo, up, dn, fgv, fgg, fmo, fup, fdn, stage_up, stage_dn,
    nrm, pad, phase, cv, hid, st, st_all,
    acc, resid, nm_all, act, fin,
    sbo1, sbi1, rdo1, rdi1, sbo2, sbi2, rdo2, rdi2,
    hsem, ws, wr, lsem, tsem, nsem, ssem, rsem, dsem, fsem,
):
    f, t = lax.axis_index("fs"), lax.axis_index("tp")
    x, y = lax.rem(f, 2), lax.rem(lax.div(f, 2), 2)
    zp, zh = lax.rem(lax.div(f, 4), 2), lax.div(f, 8)
    mid = lax.rem(zp + zh, 2)
    sib = 1 - t
    L = tok.shape[0] // 2
    half = ng * L
    width = tok.shape[1]
    chans = fgv.shape[1]
    hidden = fup.shape[1]
    depth = gv.shape[0]
    sends = []

    def flip(coord, bit):
        return 1 - coord if bit else coord

    def chip(dq):
        return flip(mid, dq // 2) * 2 + flip(x, dq % 2)

    def fs_of(dq, do):
        return flip(zh, do // 2) * 8 + flip(zp, (dq // 2 + do // 2) % 2) * 4 + flip(y, do % 2) * 2 + flip(x, dq % 2)

    def seat(dq):
        return flip(y, dq // 2) * 2 + flip(x, dq % 2)

    def seat_fs(dq, do=0):
        return zh * 8 + zp * 4 + flip(y, dq // 2) * 2 + flip(x, dq % 2)

    p, s = chip(0), seat(0)
    near, mate = fs_of(2, 0), fs_of(0, 2)
    z = zh * 2 + zp
    z_near = zh * 2 + 1 - zp
    z_mate, z_far = (1 - zh) * 2 + zh, (1 - zh) * 2 + 1 - zh
    outer, inner = mid == 0, mid == 1

    def remote(src, dst, s_sem, r_sem, device):
        return pltpu.make_async_remote_copy(
            src_ref=src, dst_ref=dst, send_sem=s_sem, recv_sem=r_sem,
            device_id=device, device_id_type=MESH,
        )

    def push(*args):
        copy = remote(*args)
        copy.start()
        sends.append(copy)

    def arrived(dst, s_sem, r_sem):
        remote(dst, dst, s_sem, r_sem, (f, sib)).wait_recv()

    loads = [
        pltpu.make_async_copy(src, dst, hsem.at[i])
        for i, (src, dst) in enumerate(((gv_in, gv), (gg_in, gg), (mo_in, mo), (up_in, up), (dn_in, dn)))
    ]
    for load in loads:
        load.start()
    barrier = pltpu.get_barrier_semaphore()
    peers = [(seat_fs(dq), u) for dq in range(1, ng) for u in (t, sib)]
    peers += [(f, sib), (near, t), (fs_of(3, 0), t), (mate, t)]
    for peer in peers:
        pl.semaphore_signal(barrier, inc=1, device_id=peer, device_id_type=MESH)

    weights = (
        (lambda q: gv.at[:, rows_at(q * chans, chans)], lambda g: fgv.at[rows_at(g * depth, depth), :]),
        (lambda q: gg.at[:, rows_at(q * chans, chans)], lambda g: fgg.at[rows_at(g * depth, depth), :]),
        (lambda q: mo.at[rows_at(q * chans, chans), :], lambda g: fmo.at[:, rows_at(g * depth, depth)]),
        (lambda q: up.at[:, rows_at(q * hidden, hidden)], lambda g: fup.at[rows_at(g * depth, depth), :]),
        (lambda q: dn.at[rows_at(q * hidden, hidden), :], lambda g: fdn.at[:, rows_at(g * depth, depth)]),
    )

    stage = (stage_up, stage_dn)

    def parts(op):
        kind, a, dq = op[0], int(op[1]), int((op + "0")[2])
        src, dst = weights[a]
        part, place = (seat, seat_fs) if a < 3 else (chip, fs_of)

        def mk(s_at, r_at, piece, to, own=None):
            return remote(piece if own is None else own, piece, ws.at[a, s_at], wr.at[a, r_at], (to, t))

        if kind == "P":
            return [], [mk(dq, dq, dst(f), place(dq, 0), src(part(dq)))]
        if kind == "X":
            return [], [mk(0, 0, stage[a - 3], fs_of(1, 0), src(chip(3)))]
        if kind == "D":
            return [mk(0, 0, stage[a - 3], f)], [mk(3, 3, dst(fs_of(1, 0)), near, stage[a - 3])]
        if kind == "W":
            return [mk(0, i, dst(place(i, 0)), f) for i in (1, 2, 3)], []
        if kind in "YGZ":
            do = 2 if kind == "Z" else 1
            piece = dst(fs_of(dq, 0))
            come = [mk(0, dq, piece, f)] if kind == "G" else []
            k = do * ng + dq
            return come, [mk(k, k, piece, fs_of(0, do), src(p) if dq == 0 else None)]
        if kind == "R":
            piece = dst(fs_of(dq, 2))
            k = 3 * ng + dq
            return [mk(0, 2 * ng + dq, piece, f)], [mk(k, k, piece, fs_of(0, 1))]
        plane = planes[a]
        if kind in "OQ":
            k, to = (4, near) if kind == "O" else (8, mate)
            own = src(part(0))
            return [], [mk(k + i, k + i, dst(place(i, 0)), to, None if i else own) for i in ((1, 2, 3) if dq else (0,))]
        if kind == "N":
            return [mk(0, 4 + i, dst(line_fs(z_near, i)), f) for i in range(4)], [mk(12, 12, plane(z_near), mate)]
        if kind == "M":
            return [mk(0, 8 + i, dst(line_fs(z_mate, i)), f) for i in range(4)], [mk(13, 13, plane(z_mate), near)]
        return [mk(0, 12, plane(z_far), f)], [mk(14, 14, plane(z_far), near)]

    def run(ops):
        for op in ops:
            come, go = parts(op)
            for copy in come:
                copy.wait_recv()
            if op[0] == "W":
                local(int(op[1])).wait()
            for copy in go:
                copy.start()

    def drain(plan):
        for ops in plan:
            for op in ops:
                for copy in parts(op)[1]:
                    copy.wait_send()

    def gap(i):
        if OUTER[i] == INNER[i]:
            run(OUTER[i])
            return
        for plan, when in ((OUTER, outer), (INNER, inner)):
            if plan[i]:
                pl.when(when)(functools.partial(run, plan[i]))

    def whole(a):
        dst = weights[a][1]
        for do in (1, 3):
            for dq in range(ng):
                arrived(dst(fs_of(dq, do)), ws.at[a, 0], wr.at[a, do * ng + dq])
        local(a).wait()

    def local(a):
        src, dst = weights[a]
        return pltpu.make_async_copy(src(s if a < 3 else p), dst(f), lsem.at[a])

    planes = (
        lambda g: fgv.at[rows_at(g * ng * depth, ng * depth), :],
        lambda g: fgg.at[rows_at(g * ng * depth, ng * depth), :],
        lambda g: fmo.at[:, rows_at(g * ng * depth, ng * depth)],
    )

    def line_fs(g, i):
        return g * ng + seat(i)

    def line_whole(a):
        for i in range(ng):
            arrived(weights[a][1](line_fs(z_near, i)), ws.at[a, 0], wr.at[a, 4 + i])
        for g, r_at in ((z_mate, 13), (z_far, 14)):
            arrived(planes[a](g), ws.at[a, 0], wr.at[a, r_at])

    first = (nrm, tsem, seat, seat_fs)
    second = (nm_all, nsem, chip, fs_of)

    def gather_start(buf, sem, part, place):
        own = buf.at[rows_at(t * half + part(0) * L, L)]
        for dq in (2, 1):
            push(own, own, sem.at[0, dq], sem.at[1, dq], (place(dq, 0), t))
        push(own, own, sem.at[2, 0], sem.at[3, 0], (f, sib))

    def gather_relay(rows, *which):
        buf, sem, part, place = rows
        for dq in which:
            block = buf.at[rows_at(t * half + part(dq) * L, L)]
            arrived(block, sem.at[0, 0], sem.at[1, dq])
            if dq == 2:
                push(block, block, sem.at[0, 3], sem.at[1, 3], (place(1, 0), t))
            push(block, block, sem.at[2, dq], sem.at[3, dq], (f, sib))

    def gather_finish(rows, *which):
        buf, sem, part, place = rows
        for dq in which:
            arrived(buf.at[rows_at(sib * half + part(dq) * L, L)], sem.at[0, 0], sem.at[3, dq])

    step = 16

    def norm_rows(load, gain, dst, start):
        def body(i, _):
            value = load(i * step).astype(F32)
            scale = lax.rsqrt(jnp.mean(value * value, axis=-1, keepdims=True) + norm_floor)
            dst[pl.ds(pl.multiple_of(start + i * step, step), step), :] = (
                value * scale * gain[...]
            ).astype(BF16)
            return 0

        lax.fori_loop(0, L // step, body, 0)

    def from_ref(ref, base):
        return lambda i: ref[pl.ds(pl.multiple_of(base + i, step), step), :]

    norm_rows(from_ref(tok, t * L), mixg, nrm, t * half + s * L)
    pl.semaphore_wait(barrier, len(peers))
    for load in loads:
        load.wait()
    gap(0)
    for a in range(5):
        local(a).start()
    gather_start(*first)
    gap(1)
    gather_relay(first, 2, 1)
    gap(2)
    gather_finish(first, 0, 1)

    @pl.when(outer)
    def _():
        line_whole(0)
        line_whole(1)

    pad[...] = jnp.zeros_like(pad)
    st[...] = jnp.zeros_like(st)
    taps_n = taps.shape[0]
    reach = taps_n // 2
    lead = (reach + 7) // 8 * 8
    reach_lead = lead - reach
    own_cols = s * chans
    eye = lax.broadcasted_iota(jnp.int32, (L, L), 0) == lax.broadcasted_iota(jnp.int32, (L, L), 1)

    def conv_half(pair_base):
        def glu_rows(u, _):
            rows = rows_at(u * half + pair_base * L, 2 * L)
            left = nrm[rows, :]
            values = jnp.dot(left, fgv[...], preferred_element_type=F32)
            gating = jnp.dot(left, fgg[...], preferred_element_type=F32)
            cv[rows, :] = (values * jax.nn.sigmoid(gating)).astype(BF16).astype(F32)
            return 0

        def conv_block(i, _):
            b = lax.rem(i, 2) * ng + pair_base + lax.div(i, 2)
            rows = rows_at(b * L, L)
            sums = jnp.zeros((L, 1), F32)
            squares = jnp.zeros((L, 1), F32)
            for c in range(chans // 128):
                at = pl.ds(c * 128, 128)
                pad[pl.ds(lead, L), :] = cv[rows, at]
                window = pad[...]
                for r in range(8):
                    partial = jnp.zeros((L + 8, 128), F32)
                    for m in range(lead // 4):
                        j = 8 * m + r - reach_lead
                        if 0 <= j < taps_n:
                            tap = taps[pl.ds(j, 1), rows_at(own_cols + c * 128, 128)]
                            partial = partial + window[8 * m : 8 * m + L + 8] * tap
                    phase[r] = partial
                total = phase[0, pl.ds(0, L), :]
                for r in range(1, 8):
                    total = total + phase[r, pl.ds(r, L), :]
                cv[rows, at] = total
                sums = sums + jnp.sum(total, axis=1, keepdims=True)
                squares = squares + jnp.sum(total * total, axis=1, keepdims=True)
            st[b, pl.ds(0, 1), :] = jnp.sum(jnp.where(eye, sums, 0.0), axis=0, keepdims=True)
            st[b, pl.ds(1, 1), :] = jnp.sum(jnp.where(eye, squares, 0.0), axis=0, keepdims=True)
            return 0

        lax.fori_loop(0, 2, glu_rows, 0)
        lax.fori_loop(0, ng, conv_block, 0)

    conv_half(y * 2)
    gather_relay(first, 3)
    gap(3)
    gather_finish(first, 2, 3)
    conv_half((1 - y) * 2)

    slots = [(dq, du) for dq in range(ng) for du in range(2) if (dq, du) != (0, 0)]
    for dq, du in slots:
        push(
            st, st_all.at[dq * 2 + du],
            ssem.at[0, dq * 2 + du], ssem.at[1, dq * 2 + du],
            (seat_fs(dq), t if du == 0 else sib),
        )
    gap(4)
    for dq, du in slots:
        arrived(st_all.at[dq * 2 + du], ssem.at[0, 0], ssem.at[1, dq * 2 + du])

    def hidden_block(b, _):
        rows = rows_at(b * L, L)
        total = st[b]
        for dq, du in slots:
            total = total + st_all[dq * 2 + du, b]
        count = chans * ng * 2
        sums = jnp.sum(jnp.where(eye, total[0:1, :], 0.0), axis=1, keepdims=True)
        squares = jnp.sum(jnp.where(eye, total[1:2, :], 0.0), axis=1, keepdims=True)
        centre = sums / count
        spread = squares / count - centre * centre
        value = (cv[rows, :] - centre) * lax.rsqrt(spread + norm_floor)
        value = value * chg[:, rows_at(own_cols, chans)]
        hid[rows, :] = (value * jax.nn.sigmoid(value)).astype(BF16)
        return 0

    lax.fori_loop(0, 2 * ng, hidden_block, 0)

    cols = 512
    span = 32
    chunks = [pl.ds(n * cols, cols) for n in range(width // cols)]

    def over_rows(body):
        def go(i, _):
            body(pl.multiple_of(i * span, span))
            return 0

        lax.fori_loop(0, L // span, go, 0)

    def mix_partial(n, dq):
        at, base = chunks[n], seat(dq) * L

        def add(i):
            row = pl.ds(pl.multiple_of(base + i, span), span)
            total = acc[row, at] + sbi1[row, at].astype(F32)
            if dq == 2:
                total = total + rdi1[2, pl.ds(i, span), at].astype(F32)
            rdo1[row, at] = total.astype(BF16)

        over_rows(add)
        push(
            rdo1.at[rows_at(base, L), at], rdi1.at[dq - 1, :, at],
            rsem.at[0, dq, n], rsem.at[1, dq, n], (seat_fs(2 if dq == 2 else 1), t),
        )

    def reduce_mixed():
        for n, at in enumerate(chunks):
            sbo1[:, at] = jnp.dot(
                hid[rows_at(sib * half, half), :], fmo[:, at], preferred_element_type=F32
            ).astype(BF16)
            push(sbo1.at[:, at], sbi1.at[:, at], rsem.at[0, 0, n], rsem.at[1, 0, n], (f, sib))

        def mine(n, _):
            at = rows_at(n * cols, cols)
            acc[:, at] = jnp.dot(
                hid[rows_at(t * half, half), :], fmo[:, at], preferred_element_type=F32
            )
            return 0

        lax.fori_loop(0, width // cols, mine, 0)
        for dq in (3, 1):
            for n, at in enumerate(chunks):
                if dq == 3:
                    arrived(sbi1.at[:, at], rsem.at[0, 0, 0], rsem.at[1, 0, n])
                mix_partial(n, dq)
        gap(6)
        for n, at in enumerate(chunks):
            arrived(rdi1.at[2, :, at], rsem.at[0, 0, 0], rsem.at[1, 3, n])
            mix_partial(n, 2)

    def reduced(i):
        at = pl.ds(pl.multiple_of(s * L + i * step, step), step)
        total = acc[at, :] + sbi1[at, :].astype(F32)
        for dq in (1, 2):
            total = total + rdi1[dq - 1, pl.ds(pl.multiple_of(i * step, step), step), :].astype(F32)
        return total.astype(BF16).astype(F32)

    @pl.when(outer)
    def _():
        line_whole(2)

    gap(5)
    reduce_mixed()
    gap(7)
    for dq in (1, 2):
        for n, at in enumerate(chunks):
            arrived(rdi1.at[dq - 1, :, at], rsem.at[0, 0, 0], rsem.at[1, dq, n])

    def resid_rows(i, _):
        at = pl.ds(pl.multiple_of(i * step, step), step)
        own = tok[pl.ds(pl.multiple_of(t * L + i * step, step), step), :].astype(F32)
        value = own + reduced(i)
        resid[at, :] = value
        scale = lax.rsqrt(jnp.mean(value * value, axis=-1, keepdims=True) + norm_floor)
        nm_all[pl.ds(pl.multiple_of(t * half + p * L + i * step, step), step), :] = (
            value * scale * mlpg[...]
        ).astype(BF16)
        return 0

    lax.fori_loop(0, L // step, resid_rows, 0)
    gather_start(*second)
    gap(8)
    gather_relay(second, 2)
    gap(9)
    gather_relay(second, 1, 3)
    gap(10)
    whole(3)

    def up_half(u):
        def body(n, _):
            at = rows_at(n * 256, 256)
            value = jnp.dot(
                nm_all[rows_at(u * half, half), :], fup[:, at], preferred_element_type=F32
            )
            value = jnp.maximum(value, 0.0)
            act[rows_at(u * half, half), at] = (value * value).astype(BF16)
            return 0

        lax.fori_loop(0, hidden // 256, body, 0)

    gap(11)
    up_half(t)
    gap(12)
    gather_finish(second, 0, 1, 2, 3)
    up_half(sib)

    pair = 2 * depth
    def pair_at(g, j):
        return rows_at((flip(zh, g // 2) * 8 + j * 4 + flip(y, g % 2) * 2) * depth, pair)

    def down_group(g):
        def theirs(j, _):
            at = pair_at(g, j)
            sbo2[:, at] = jnp.dot(
                act[rows_at(sib * half, half), :], fdn[:, at], preferred_element_type=F32
            ).astype(BF16)
            return 0

        def mine(j, _):
            at = pair_at(g, j)
            acc[:, at] = jnp.dot(
                act[rows_at(t * half, half), :], fdn[:, at], preferred_element_type=F32
            )
            return 0

        lax.fori_loop(0, 2, theirs, 0)
        for j in range(2):
            at = pair_at(g, j)
            push(sbo2.at[:, at], sbi2.at[:, at], dsem.at[0, g * 2 + j, 0], dsem.at[1, g * 2 + j, 0], (f, sib))
        lax.fori_loop(0, 2, mine, 0)
        for j in range(2):
            arrived(sbi2.at[:, pair_at(g, j)], dsem.at[0, 0, 0], dsem.at[1, g * 2 + j, 0])
        for dq in (3, 1):
            for j in range(2):
                pass_partial(g, j, dq)

    def pass_partial(g, j, dq):
        at, base = pair_at(g, j), chip(dq) * L

        def add(i):
            row = pl.ds(pl.multiple_of(base + i, span), span)
            total = acc[row, at] + sbi2[row, at].astype(F32)
            if dq == 2:
                total = total + rdi2[2, pl.ds(i, span), at].astype(F32)
            rdo2[row, at] = total.astype(BF16)

        over_rows(add)
        push(
            rdo2.at[rows_at(base, L), at], rdi2.at[dq - 1, :, at],
            dsem.at[0, g * 2 + j, dq], dsem.at[1, g * 2 + j, dq], (fs_of(2 if dq == 2 else 1, 0), t),
        )

    def down_near(g):
        for j in range(2):
            arrived(rdi2.at[2, :, pair_at(g, j)], dsem.at[0, 0, 0], dsem.at[1, g * 2 + j, 3])
            pass_partial(g, j, 2)

    def down_final(g):
        for j in range(2):
            at = pair_at(g, j)
            for dq in (1, 2):
                arrived(rdi2.at[dq - 1, :, at], dsem.at[0, 0, 0], dsem.at[1, g * 2 + j, dq])

            def finish(i):
                row = pl.ds(pl.multiple_of(p * L + i, span), span)
                here = pl.ds(i, span)
                total = acc[row, at] + sbi2[row, at].astype(F32)
                total = total + rdi2[0, here, at].astype(F32) + rdi2[1, here, at].astype(F32)
                value = (resid[here, at] + total.astype(BF16).astype(F32)).astype(BF16)
                fin[0, here, at] = value
                out[pl.ds(pl.multiple_of(t * L + i, span), span), at] = value

            over_rows(finish)
            push(fin.at[0, :, at], fin.at[1, :, at], fsem.at[0, g * 2 + j], fsem.at[1, g * 2 + j], (f, sib))

    def down_copy(g):
        for j in range(2):
            at = pair_at(g, j)
            arrived(fin.at[1, :, at], fsem.at[0, 0], fsem.at[1, g * 2 + j])
            out[rows_at(sib * L, L), at] = fin[1, :, at]

    def down_wait(do):
        for dq in range(ng):
            arrived(weights[4][1](fs_of(dq, do)), ws.at[4, 0], wr.at[4, do * ng + dq])

    local(4).wait()
    gap(13)
    down_group(0)
    gap(14)
    down_wait(1)
    down_group(1)
    down_near(0)
    down_group(2)
    down_near(1)
    down_final(0)
    down_wait(3)
    down_group(3)
    down_near(2)
    down_final(1)
    down_copy(0)
    down_near(3)
    down_final(2)
    down_copy(1)
    down_final(3)
    down_copy(2)
    down_copy(3)
    for copy in sends:
        copy.wait_send()
    for plan, when in ((OUTER, outer), (INNER, inner)):
        pl.when(when)(functools.partial(drain, plan))


def fused_device(ng, nz, tokens, mix_gain, glu_value, glu_gate, conv_taps, chan_gain, mix_out, mlp_gain, up_weight, down_weight):
    rows, width = tokens.shape
    fs = ng * nz
    L = rows // 2
    half = ng * L
    chans = glu_value.shape[1] // ng
    hidden = up_weight.shape[1] // ng
    depth = glu_value.shape[0]
    blocks = 2 * ng
    vm = pltpu.VMEM
    dma = pltpu.SemaphoreType.DMA
    reduce_bufs = [
        vm((half, width), BF16), vm((half, width), BF16), vm((half, width), BF16),
        vm((ng - 1, L, width), BF16),
    ]
    held = (2, 3, 6, 8, 9)
    scratch = [
        *(vm(w.shape, BF16) for w in (glu_value, glu_gate, mix_out, up_weight, down_weight)),
        vm((fs * depth, chans), BF16), vm((fs * depth, chans), BF16), vm((chans, width), BF16),
        vm((fs * depth, hidden), BF16), vm((hidden, width), BF16),
        vm((depth, hidden), BF16), vm((hidden, depth), BF16),
        vm((2 * half, width), BF16),
        vm((L + 32, 128), F32), vm((8, L + 8, 128), F32), vm((2 * half, chans), F32), vm((2 * half, chans), BF16),
        vm((blocks, 8, L), F32), vm((blocks, blocks, 8, L), F32),
        vm((half, width), F32), vm((L, width), F32), vm((2 * half, width), BF16),
        vm((2 * half, hidden), BF16), vm((2, L, width), BF16),
        *reduce_bufs, *reduce_bufs,
        dma((5,)), dma((5, fs)), dma((5, fs)), dma((5,)), dma((4, ng)), dma((4, ng)),
        dma((2, blocks)), dma((2, ng, 4)), dma((2, 2 * ng, 4)), dma((2, 2 * ng)),
    ]
    return pl.pallas_call(
        functools.partial(layer_kernel, ng),
        out_shape=jax.ShapeDtypeStruct((rows, width), BF16),
        in_specs=[pl.BlockSpec(memory_space=pl.ANY if i in held else vm) for i in range(10)],
        out_specs=pl.BlockSpec(memory_space=vm),
        scratch_shapes=scratch,
        compiler_params=pltpu.CompilerParams(
            collective_id=0, has_side_effects=True, vmem_limit_bytes=60 * 1024 * 1024
        ),
    )(
        tokens, mix_gain[None], glu_value, glu_gate, conv_taps, chan_gain[None], mix_out,
        mlp_gain[None], up_weight, down_weight,
    )


def per_device(*args):
    tokens, glu_value, conv_taps = args[0], args[2], args[4]
    fs, tp = lax.axis_size("fs"), lax.axis_size("tp")
    group = 4
    fits = (
        tp == 2
        and fs == group * 4
        and tokens.shape[0] == 2 * LEN
        and glu_value.shape[0] % 128 == 0
        and conv_taps.shape[1] % (group * 128) == 0
        and conv_taps.shape[0] <= 31
    )
    if fits:
        return fused_device(group, fs // group, *args)
    return plain_device(*args)


def solution(mesh):
    in_specs = (
        P("fs", None),
        P(),
        P("fs", "tp"),
        P("fs", "tp"),
        P(None, "tp"),
        P("tp"),
        P("tp", "fs"),
        P(),
        P("fs", "tp"),
        P("tp", "fs"),
    )
    out_specs = P("fs", None)
    return jax.shard_map(
        per_device, mesh=mesh, in_specs=in_specs, out_specs=out_specs, check_vma=False
    )
```
